256 devices in a mesh: grp: 2 (over y), sp: 16 (over z), fs: 4 (over x), tp: 2 (over core).
Axes of the slice: x: 4, y: 2, z: 16, core: 2. Of those that a mesh axis runs over, the one named last changes fastest.
The devices are a block of a 4x16x16 slice.
Arguments:
- tokens: bfloat16 [8, 8192, 2048], P(('grp', 'fs'), ('sp', 'tp')), parts along dimension 0, may hold values from -6 to 6
- norm_gain: float32 [2048], replicated, may hold values from 0.1 to 1.9
- w_bgate: bfloat16 [2048, 2048], P(('sp', 'fs'), 'tp'), may hold values from -0.125 to 0.125
- w_cgate: bfloat16 [2048, 2048], P(('sp', 'fs'), 'tp'), may hold values from -0.125 to 0.125
- w_conv_in: bfloat16 [2048, 2048], P(('sp', 'fs'), 'tp'), may hold values from -0.125 to 0.125
- conv_taps: bfloat16 [3, 2048], P(None, 'tp'), may hold values from -3.5 to 3.5
- w_query: bfloat16 [2048, 2048], P(('sp', 'fs'), 'tp'), may hold values from -0.13258252 to 0.13258252
- w_key: bfloat16 [2048, 256], P(('sp', 'fs'), 'tp'), may hold values from -4.02167 to 4.02167
- w_value: bfloat16 [2048, 256], P(('sp', 'fs'), 'tp'), may hold values from -0.125 to 0.125
- sink_logits: float32 [32], P('tp'), may hold values from 1 to 6
- conv_out_weight: bfloat16 [2048, 2048], P('tp', ('sp', 'fs')), may hold values from -0.125 to 0.125
- attn_out_weight: bfloat16 [2048, 2048], P('tp', ('sp', 'fs')), may hold values from -0.75 to 0.75
Outputs:
- mixed: bfloat16 [8, 8192, 2048], P(('grp', 'fs'), ('sp', 'tp')), parts along dimension 0
The draws below stay inside these ranges and needn't reach their ends.
There are 2 independent parts, one for each index of `grp`. The reference program is written for one: setup_inputs(seed, part) draws one part's arguments, and reference() takes and returns one part's arrays. A program takes and returns all parts, laid end to end along the dimension named above; an argument that names none is the same for every part. Nothing has to cross between parts.
All inputs are finite; a program needn't handle non-finite values.
Results may differ from the reference program's by a relative error of at most 0.014.
The reference program's roundings to bfloat16 on the way count: a program that leaves them out, or rounds other values in their place, can miss the bound.
Values may be sent and summed in bfloat16 or wider, within the bound.
No kernel may reach another device: no remote copies, remote signals or barrier semaphores. Data moves between devices by JAX's collectives and lax.ppermute only.
A program may use at most 128 MiB of HBM per device.

```python
import jax
import jax.numpy as jnp
from jax import lax

D = 2048
CONV = 2048
HEADS = 32
KV_HEADS = 4
HEAD = 64
WINDOW = 128
TAPS = 3
ATTN_Q = 2048
ATTN_KV = 256
SEQS = 4
LENGTH = 8192
N_TP = 2


def query_matrix(key):
    raw = jax.random.normal(jax.random.fold_in(key, 31), (D, ATTN_Q), jnp.float32)
    return jnp.clip(raw, -6.0, 6.0) / jnp.sqrt(jnp.float32(D))


def draw_w_query(key, part):
    return query_matrix(key).astype(jnp.bfloat16)


def draw_w_key(key, part):
    raw = jax.random.normal(jax.random.fold_in(key, 32), (D, ATTN_KV), jnp.float32)
    noise = jnp.clip(raw, -6.0, 6.0) / jnp.sqrt(jnp.float32(D))
    return noise.astype(jnp.bfloat16)


def draw_tokens(key, part):
    base = jnp.clip(jax.random.normal(jax.random.fold_in(key, 41), (SEQS, LENGTH, D), jnp.float32), -6.0, 6.0)
    return base.astype(jnp.bfloat16)


def steps_of(rng, shape, shards, smallest, high):
    gain = 1.0
    for dim, parts in shards:
        draws = jax.random.uniform(jax.random.fold_in(jax.random.fold_in(rng, 6), dim), (parts,), jnp.float32, smallest / len(shards), high / len(shards))
        gain = gain * jnp.repeat(jnp.exp(draws), shape[dim] // parts).reshape((-1,) + (1,) * (len(shape) - 1 - dim))
    return gain


def normal_values(own_key, shape, spread, bound, pieces=(), kind=jnp.bfloat16):
    array = jax.random.normal(own_key, shape, jnp.float32) * spread
    if len(pieces) > 0:
        array = steps_of(own_key, shape, pieces, -0.22, 0.18) * array
    return jnp.clip(array, min=-bound, max=bound).astype(kind)


def setup_inputs(seed: int = 0, part: int = 0) -> dict:
    key_list = jax.random.split(jax.random.key(seed), 13)
    own_keys = jax.random.split(jax.random.fold_in(key_list[12], part), 13)
    return {
        "tokens": draw_tokens(jax.random.fold_in(jax.random.fold_in(key_list[12], part), 71), part),
        "norm_gain": jnp.clip(1.0 + 0.18 * jax.random.normal(key_list[1], (D,), jnp.float32), 0.1, 1.9),
        "w_bgate": normal_values(key_list[2], (D, CONV), D ** -0.5, 0.125, ((0, 64), (1, 2))),
        "w_cgate": normal_values(key_list[3], (D, CONV), D ** -0.5, 0.125, ((0, 64), (1, 2))),
        "w_conv_in": normal_values(key_list[4], (D, CONV), D ** -0.5, 0.125, ((0, 64), (1, 2))),
        "conv_taps": normal_values(key_list[5], (TAPS, CONV), TAPS ** -0.5, 3.5, ((1, 2),)),
        "w_query": draw_w_query(jax.random.fold_in(key_list[12], 71), part),
        "w_key": draw_w_key(jax.random.fold_in(key_list[12], 71), part),
        "w_value": normal_values(key_list[8], (D, ATTN_KV), D ** -0.5, 0.125, ((0, 64), (1, 2))),
        "sink_logits": jnp.clip(1.0 + 5.0 * jax.random.uniform(key_list[9], (HEADS,), jnp.float32) ** steps_of(key_list[9], (HEADS,), ((0, 2),), -0.2, 0.2), 1.0, 6.0),
        "conv_out_weight": normal_values(key_list[10], (CONV, D), CONV ** -0.5, 0.125, ((0, 2), (1, 64))),
        "attn_out_weight": normal_values(key_list[11], (ATTN_Q, D), (ATTN_Q // 32) ** -0.5, 0.75, ((0, 2), (1, 64))),
    }


epsilon = 1e-06

def window_attention(queries, key_rows, value_rows, sink_logits):
    length = queries.shape[0]
    blocks = length // WINDOW
    groups = HEADS // KV_HEADS
    query_blocks = queries.astype(jnp.float32).reshape(blocks, WINDOW, KV_HEADS, groups, HEAD)
    zero_rows = jnp.zeros((WINDOW, ATTN_KV), jnp.float32)
    key_all = jnp.concatenate([zero_rows, key_rows.astype(jnp.float32)], 0)
    value_all = jnp.concatenate([zero_rows, value_rows.astype(jnp.float32)], 0)
    key_band = jnp.concatenate([key_all[:length].reshape(blocks, WINDOW, KV_HEADS, HEAD), key_all[WINDOW:].reshape(blocks, WINDOW, KV_HEADS, HEAD)], 1)
    value_band = jnp.concatenate([value_all[:length].reshape(blocks, WINDOW, KV_HEADS, HEAD), value_all[WINDOW:].reshape(blocks, WINDOW, KV_HEADS, HEAD)], 1)
    scores = jnp.einsum('nqhgd,nkhd->nhgqk', query_blocks, key_band) / jnp.sqrt(jnp.float32(HEAD))
    block_ids = jnp.arange(blocks)[:, None, None]
    query_pos = block_ids * WINDOW + jnp.arange(WINDOW)[None, :, None]
    key_pos = (block_ids - 1) * WINDOW + jnp.arange(2 * WINDOW)[None, None, :]
    allowed = (key_pos >= 0) & (key_pos <= query_pos) & (query_pos - key_pos < WINDOW)
    scores = jnp.where(allowed[:, None, None], scores, -jnp.inf)
    sink_grid = sink_logits.astype(jnp.float32).reshape(1, KV_HEADS, groups, 1, 1)
    peak_score = jnp.maximum(lax.optimization_barrier(jnp.max(scores, axis=-1, keepdims=True)), sink_grid)
    weights = jnp.exp(scores - peak_score)
    denominator = lax.optimization_barrier(jnp.sum(weights, axis=-1, keepdims=True)) + jnp.exp(sink_grid - peak_score)
    probabilities = (weights / denominator).astype(jnp.bfloat16)
    attended = jnp.einsum('nhgqk,nkhd->nqhgd', probabilities.astype(jnp.float32), value_band)
    return attended.astype(jnp.bfloat16).reshape(length, ATTN_Q)

def one_sequence(tokens, norm_gain, w_bgate, w_cgate, w_conv_in, conv_taps, w_query, w_key, w_value, sink_logits, conv_out_weight, attn_out_weight):
    widened = tokens.astype(jnp.float32)
    normed = (widened * lax.rsqrt(lax.optimization_barrier(jnp.mean(widened * widened, axis=-1, keepdims=True)) + epsilon) * norm_gain).astype(jnp.bfloat16)

    def project(weight):
        return jnp.dot(normed, weight, preferred_element_type=jnp.float32).astype(jnp.bfloat16)
    out_gate = project(w_bgate)
    in_gate = project(w_cgate)
    conv_input = project(w_conv_in)
    queries = project(w_query)
    key_rows = project(w_key)
    value_rows = project(w_value)
    length = tokens.shape[0]
    gated = (in_gate.astype(jnp.float32) * conv_input.astype(jnp.float32)).astype(jnp.bfloat16)
    padded = jnp.concatenate([jnp.zeros((TAPS - 1, CONV), jnp.bfloat16), gated], 0)
    taps_wide = conv_taps.astype(jnp.float32)
    convolved = padded[0:length].astype(jnp.float32) * taps_wide[0]
    for which in range(1, TAPS):
        convolved = convolved + padded[which:which + length].astype(jnp.float32) * taps_wide[which]
    conv_branch = (out_gate.astype(jnp.float32) * convolved).astype(jnp.bfloat16)
    attended = window_attention(queries, key_rows, value_rows, sink_logits)
    conv_parts = conv_branch.reshape(length, N_TP, CONV // N_TP)
    attn_parts = attended.reshape(length, N_TP, ATTN_Q // N_TP)
    conv_weight_parts = conv_out_weight.reshape(N_TP, CONV // N_TP, D)
    attn_weight_parts = attn_out_weight.reshape(N_TP, ATTN_Q // N_TP, D)
    running = jnp.zeros((length, D), jnp.float32)
    for member in range(N_TP):
        partial_value = jnp.dot(conv_parts[:, member], conv_weight_parts[member], preferred_element_type=jnp.float32)
        partial_value = partial_value + jnp.dot(attn_parts[:, member], attn_weight_parts[member], preferred_element_type=jnp.float32)
        rounded = lax.optimization_barrier(partial_value.astype(jnp.bfloat16))
        running = running + rounded.astype(jnp.float32)
    return running.astype(jnp.bfloat16)

def reference(tokens, norm_gain, w_bgate, w_cgate, w_conv_in, conv_taps, w_query, w_key, w_value, sink_logits, conv_out_weight, attn_out_weight):
    results = []
    for sequence in range(SEQS):
        results.append(one_sequence(tokens[sequence], norm_gain, w_bgate, w_cgate, w_conv_in, conv_taps, w_query, w_key, w_value, sink_logits, conv_out_weight, attn_out_weight))
    return jnp.stack(results, 0)
```

```python
import functools

import jax
import jax.numpy as jnp
from jax import lax
from jax.experimental import pallas as pl
from jax.experimental.pallas import tpu as pltpu
from jax.sharding import PartitionSpec as P

HEAD = 64
WINDOW = 128
TAPS = 3
EPSILON = 1e-06


ANY = pl.BlockSpec(memory_space=pl.ANY)
SMEM = pl.BlockSpec(memory_space=pltpu.SMEM)
VMEM = pl.BlockSpec(memory_space=pltpu.VMEM)


def ring(array, axis, by):
    size = lax.axis_size(axis)
    return lax.ppermute(array, axis, [(i, (i + by) % size) for i in range(size)])


def swapped(array):
    return lax.ppermute(array, "tp", [(0, 1), (1, 0)])


def gather_streams(streams, axis):
    size = lax.axis_size(axis)
    rows = streams[0].shape[0]
    half = rows // 2
    ahead, behind = list(streams), list(streams)
    pieces = [[(0, 0, s)] for s in streams]
    for step in range(1, size // 2 + 1):
        for k in range(len(streams)):
            if step == size // 2:
                pieces[k].append((-step, 0, ring(ahead[k][:half], axis, 1)))
                pieces[k].append((-step, half, ring(behind[k][half:], axis, -1)))
            else:
                ahead[k] = ring(ahead[k], axis, 1)
                behind[k] = ring(behind[k], axis, -1)
                pieces[k].append((-step, 0, ahead[k]))
                pieces[k].append((step, 0, behind[k]))
    return pieces


def piece_copies(spots, refs, dst, src_cols, dst_cols, place, sems, first, block, size):
    copies = []
    for i, ((offset, start, rows), ref) in enumerate(zip(spots, refs)):
        row = pl.multiple_of(lax.rem(place + (offset + size), size) * block + start, 64)
        copies.append(
            pltpu.make_async_copy(
                ref.at[:, src_cols],
                dst.at[pl.ds(row, rows), dst_cols],
                sems.at[first + i],
            )
        )
    return copies


def edge_kernel(spots, size, block, feat, idx, *refs):
    count = len(spots)
    mine, theirs = refs[:4], refs[4:8]
    a_refs, b_refs = refs[8 : 8 + count], refs[8 + count : 8 + 2 * count]
    out, xs, wkv, wci, sems = refs[8 + 2 * count :]
    core, place = idx[0], idx[1]
    cols = wkv.shape[1]
    wide = wci.shape[1]
    copies = piece_copies(
        spots, a_refs, wkv, pl.ds(feat, cols), pl.ds(0, cols), place, sems, 4, block, size
    ) + piece_copies(
        spots, b_refs, wci, pl.ds(feat, wide), pl.ds(0, wide), place, sems, 4 + count, block, size
    )

    def rows_of(ref, s):
        start = ref.shape[0] - WINDOW
        return pltpu.make_async_copy(
            ref.at[pl.ds(start, WINDOW), :], xs.at[pl.ds(s * WINDOW, WINDOW), :], sems.at[s]
        )

    for c in copies:
        c.start()

    @pl.when(core == 1)
    def _():
        for s in range(4):
            rows_of(mine[s], s).start()

    @pl.when(core == 0)
    def _():
        for s in range(4):
            rows_of(theirs[s], s).start()

    for s in range(4):
        rows_of(mine[s], s).wait()
    for c in copies[:count]:
        c.wait()
    x = xs[...]
    kv = jnp.dot(x, wkv[...], preferred_element_type=jnp.float32).astype(jnp.bfloat16)
    for c in copies[count:]:
        c.wait()
    last = jnp.concatenate(
        [xs[(s + 1) * WINDOW - 16 : (s + 1) * WINDOW, :] for s in range(4)], axis=0
    )
    ci = jnp.dot(last, wci[...], preferred_element_type=jnp.float32).astype(jnp.bfloat16)
    ci = ci.astype(jnp.float32)
    gated = (ci[:, : wide // 2] * ci[:, wide // 2 :]).astype(jnp.bfloat16)
    for s in range(4):
        out[s, 0:WINDOW, :] = kv[s * WINDOW : (s + 1) * WINDOW]
        out[s, WINDOW : WINDOW + 16, :] = gated[s * 16 : (s + 1) * 16, :128]
        out[s, WINDOW + 16 : WINDOW + 32, :] = gated[s * 16 : (s + 1) * 16, 128:]


def project_kernel(spots, size, block, feat, wide, idx, *refs):
    count = len(spots)
    mine, theirs = refs[:5], refs[5:10]
    a_refs, b_refs = refs[10 : 10 + count], refs[10 + count : 10 + 2 * count]
    out, wout, xs, ws, sems = refs[10 + 2 * count :]
    core, place = idx[0], idx[1]
    step = pl.program_id(0)
    half = xs.shape[1] // 2
    a_cols = ws.shape[1] - wide
    oc = wout.shape[1]
    w_copies = piece_copies(
        spots, b_refs, ws, pl.ds(0, wide), pl.ds(0, wide), place, sems, 20, block, size
    ) + piece_copies(
        spots, a_refs, ws, pl.ds(0, a_cols), pl.ds(wide, a_cols), place, sems, 20 + count, block, size
    )
    o_copies = piece_copies(
        spots, a_refs, wout, pl.ds(a_cols, oc), pl.ds(0, oc), place, sems, 20 + 2 * count, block, size
    )

    def x_copies(s):
        made = []
        for which, (group, base) in enumerate(
            ((mine, core * half), (theirs, (1 - core) * half))
        ):
            parts = ((group[0], 0), (group[1], half // 2)) if s == 0 else ((group[s + 1], 0),)
            for j, (ref, at) in enumerate(parts):
                row = pl.multiple_of(base + at, 128)
                made.append(
                    pltpu.make_async_copy(
                        ref, xs.at[s, pl.ds(row, ref.shape[0]), :], sems.at[4 * s + 2 * which + j]
                    )
                )
        return made

    @pl.when(step == 0)
    def _():
        for c in x_copies(0) + w_copies:
            c.start()
        for s in range(1, 4):
            for c in x_copies(s):
                c.start()
        for c in o_copies:
            c.start()
        for c in w_copies:
            c.wait()

    for s in range(4):

        @pl.when(step == s)
        def _():
            for c in x_copies(s):
                c.wait()
            if s == 3:
                for c in o_copies:
                    c.wait()

    tile = 384

    def body(i, carry):
        col = pl.multiple_of(i * tile, 128)
        acc = jnp.dot(xs[step], ws[:, pl.ds(col, tile)], preferred_element_type=jnp.float32)
        out[0, :, pl.ds(col, tile)] = acc.astype(jnp.bfloat16)
        return carry

    lax.fori_loop(0, ws.shape[1] // tile, body, 0)


def mix_kernel(wide, idx, sinks, proj, edge, taps, wout, keep, send, acts, k4, v4):
    core, place = idx[0], idx[1]
    length = proj.shape[1]
    chans = wide // 3
    f32 = jnp.float32
    out_gate = proj[0, :, 0:chans].astype(f32)
    gated = (
        proj[0, :, chans : 2 * chans].astype(f32) * proj[0, :, 2 * chans : 3 * chans].astype(f32)
    ).astype(jnp.bfloat16)
    gated = gated.astype(f32)
    tail = jnp.concatenate(
        [edge[0, WINDOW : WINDOW + 16, :], edge[0, WINDOW + 16 : WINDOW + 32, :]], axis=1
    ).astype(f32)
    before2, before1 = tail[14:15, :], tail[15:16, :]
    row = lax.broadcasted_iota(jnp.int32, (length, chans), 0)
    one = jnp.where(row == 0, before1, pltpu.roll(gated, 1, 0))
    two = jnp.where(row == 0, before2, jnp.where(row == 1, before1, pltpu.roll(gated, 2, 0)))
    t = taps[...].astype(f32)
    convolved = two * t[0:1] + one * t[1:2] + gated * t[2:3]
    acts[:, 0:chans] = (out_gate * convolved).astype(jnp.bfloat16)

    q_at, kv_at = wide, wide + chans
    r = lax.broadcasted_iota(jnp.int32, (2 * HEAD, chans), 0)
    c = lax.broadcasted_iota(jnp.int32, (2 * HEAD, chans), 1)
    pick_k = (r == jnp.bitwise_and(c, HEAD - 1)).astype(jnp.bfloat16)
    pick_v = (r == jnp.bitwise_and(c, HEAD - 1) + HEAD).astype(jnp.bfloat16)
    kv_before = edge[0, 0:WINDOW, :]
    kv_here = proj[0, :, kv_at : kv_at + 2 * HEAD]
    for dst, pick in ((k4, pick_k), (v4, pick_v)):
        dst[0:WINDOW, :] = jnp.dot(kv_before, pick, preferred_element_type=f32).astype(jnp.bfloat16)
        dst[WINDOW:, :] = jnp.dot(kv_here, pick, preferred_element_type=f32).astype(jnp.bfloat16)
    qi = lax.broadcasted_iota(jnp.int32, (WINDOW, 2 * WINDOW), 0)
    ki = lax.broadcasted_iota(jnp.int32, (WINDOW, 2 * WINDOW), 1)
    band = (ki > qi) & (ki <= qi + WINDOW)
    first = band & ((ki >= WINDOW) | (place > 0))
    lane = lax.broadcasted_iota(jnp.int32, (WINDOW, chans), 1)
    heads = chans // HEAD
    for n in range(length // WINDOW):
        q = proj[0, n * WINDOW : (n + 1) * WINDOW, q_at : q_at + chans]
        keys = k4[n * WINDOW : (n + 2) * WINDOW, :]
        values = v4[n * WINDOW : (n + 2) * WINDOW, :]
        allowed = first if n == 0 else band
        total = jnp.zeros((WINDOW, chans), f32)
        for h in range(heads):
            of_head = (lane >= h * HEAD) & (lane < (h + 1) * HEAD)
            qh = jnp.where(of_head, q, jnp.zeros_like(q))
            s = lax.dot_general(qh, keys, (((1,), (1,)), ((), ())), preferred_element_type=f32)
            s = jnp.where(allowed, s * (1.0 / 8.0), -jnp.inf)
            sink = sinks[h]
            m = jnp.maximum(jnp.max(s, axis=1, keepdims=True), sink)
            e = jnp.exp(s - m)
            d = jnp.sum(e, axis=1, keepdims=True) + jnp.exp(sink - m)
            p = (e / d).astype(jnp.bfloat16)
            o = jnp.dot(p, values, preferred_element_type=f32)
            total = jnp.where(of_head, o, total)
        acts[n * WINDOW : (n + 1) * WINDOW, chans:] = total.astype(jnp.bfloat16)

    half = length // 2
    tile = 512
    for dst, start in ((send, (1 - core) * half), (keep, core * half)):
        a = acts[pl.ds(pl.multiple_of(start, 128), half), :]

        def body(i, carry):
            col = pl.multiple_of(i * tile, 128)
            acc = lax.dot_general(
                a, wout[pl.ds(col, tile), :], (((1,), (1,)), ((), ())), preferred_element_type=f32
            )
            dst[:, pl.ds(col, tile)] = acc.astype(jnp.bfloat16)
            return carry

        lax.fori_loop(0, dst.shape[1] // tile, body, 0)


def added(*parts):
    total = parts[0].astype(jnp.float32)
    for p in parts[1:]:
        total = total + p.astype(jnp.float32)
    return total.astype(jnp.bfloat16)


def local(
    tokens,
    norm_gain,
    w_bgate,
    w_cgate,
    w_conv_in,
    conv_taps,
    w_query,
    w_key,
    w_value,
    sink_logits,
    conv_out_weight,
    attn_out_weight,
):
    fs = lax.axis_size("fs")
    sp = lax.axis_size("sp")
    bf16, f32 = jnp.bfloat16, jnp.float32
    rows_in = w_bgate.shape[0]
    chans = w_bgate.shape[1] // fs
    kv_heads = w_key.shape[1] // HEAD
    block = rows_in * fs
    conv_t, attn_t = conv_out_weight.T, attn_out_weight.T
    to_a, to_b = [], []
    for f in range(fs):
        cut = slice(f * chans, (f + 1) * chans)
        kv = f * kv_heads // fs
        kv_cut = slice(kv * HEAD, (kv + 1) * HEAD)
        to_a.append(
            jnp.concatenate(
                [w_query[:, cut], w_key[:, kv_cut], w_value[:, kv_cut], conv_t[:, cut], attn_t[:, cut]],
                axis=1,
            )
        )
        to_b.append(jnp.concatenate([w_bgate[:, cut], w_cgate[:, cut], w_conv_in[:, cut]], axis=1))
    a_width, b_width = to_a[0].shape[1], to_b[0].shape[1]
    packed = jnp.stack([jnp.concatenate([a, b], axis=1) for a, b in zip(to_a, to_b)])
    mine = lax.all_to_all(packed, "fs", split_axis=0, concat_axis=0, tiled=True)
    mine = mine.reshape(block, a_width + b_width)
    streams = [mine[:, :a_width], mine[:, a_width:]]

    widened = tokens[0].astype(f32)
    normed = (
        widened
        * lax.rsqrt(jnp.mean(widened * widened, axis=-1, keepdims=True) + EPSILON)
        * norm_gain
    ).astype(bf16)
    here, feats = normed.shape
    half = here // 2
    prev = ring(normed, "fs", 1)
    succ = ring(normed, "fs", -1)
    opp_a = ring(prev[:half], "fs", 1)
    opp_b = ring(succ[half:], "fs", -1)
    own_rows = [opp_a, opp_b, succ, prev, normed]
    other_rows = [swapped(a) for a in own_rows]

    pieces = gather_streams(streams, "sp")
    spots = tuple((o, s, p.shape[0]) for o, s, p in pieces[0])
    blocks_a = [p for _, _, p in pieces[0]]
    blocks_b = [p for _, _, p in pieces[1]]
    count = len(spots)
    length = 2 * here
    in_cols = chans + 2 * HEAD + b_width
    out_cols = a_width - chans - 2 * HEAD

    core, place, group = lax.axis_index("tp"), lax.axis_index("sp"), lax.axis_index("fs")
    idx = jnp.stack([core, place]).astype(jnp.int32)
    taps = lax.dynamic_slice_in_dim(conv_taps, group * chans, chans, 1)
    sinks = lax.dynamic_slice_in_dim(sink_logits, group * (chans // HEAD), chans // HEAD, 0)

    edge = pl.pallas_call(
        functools.partial(edge_kernel, spots, sp, block, chans),
        out_shape=jax.ShapeDtypeStruct((4, WINDOW + 32, 2 * HEAD), bf16),
        in_specs=[SMEM] + [ANY] * (8 + 2 * count),
        out_specs=VMEM,
        scratch_shapes=[
            pltpu.VMEM((4 * WINDOW, feats), bf16),
            pltpu.VMEM((feats, 2 * HEAD), bf16),
            pltpu.VMEM((feats, 2 * chans), bf16),
            pltpu.SemaphoreType.DMA((4 + 2 * count,)),
        ],
        cost_estimate=pl.CostEstimate(flops=600_000_000, bytes_accessed=5_000_000, transcendentals=0),
        name="edge_rows",
    )(idx, *own_rows[1:], *other_rows[1:], *blocks_a, *blocks_b)
    edge = lax.ppermute(edge, "sp", [(i, i + 1) for i in range(sp - 1)])

    proj, wout = pl.pallas_call(
        functools.partial(project_kernel, spots, sp, block, chans, b_width),
        out_shape=(
            jax.ShapeDtypeStruct((4, length, in_cols), bf16),
            jax.ShapeDtypeStruct((feats, out_cols), bf16),
        ),
        grid=(4,),
        in_specs=[SMEM] + [ANY] * (10 + 2 * count),
        out_specs=(
            pl.BlockSpec((1, length, in_cols), lambda s: (s, 0, 0)),
            pl.BlockSpec((feats, out_cols), lambda s: (0, 0)),
        ),
        scratch_shapes=[
            pltpu.VMEM((4, length, feats), bf16),
            pltpu.VMEM((feats, in_cols), bf16),
            pltpu.SemaphoreType.DMA((20 + 3 * count,)),
        ],
        cost_estimate=pl.CostEstimate(
            flops=2 * 4 * length * feats * in_cols, bytes_accessed=20_000_000, transcendentals=0
        ),
        compiler_params=pltpu.CompilerParams(dimension_semantics=("arbitrary",)),
        name="project_rows",
    )(idx, *own_rows, *other_rows, *blocks_a, *blocks_b)

    def mix(s):
        return pl.pallas_call(
            functools.partial(mix_kernel, b_width),
            out_shape=(jax.ShapeDtypeStruct((here, feats), bf16),) * 2,
            grid=(1,),
            in_specs=[
                SMEM,
                SMEM,
                pl.BlockSpec((1, length, in_cols), lambda i: (s, 0, 0)),
                pl.BlockSpec((1, WINDOW + 32, 2 * HEAD), lambda i: (s, 0, 0)),
                pl.BlockSpec((TAPS, chans), lambda i: (0, 0)),
                pl.BlockSpec((feats, out_cols), lambda i: (0, 0)),
            ],
            out_specs=(pl.BlockSpec((here, feats), lambda i: (0, 0)),) * 2,
            scratch_shapes=[
                pltpu.VMEM((length, out_cols), bf16),
                pltpu.VMEM((length + WINDOW, chans), bf16),
                pltpu.VMEM((length + WINDOW, chans), bf16),
            ],
            cost_estimate=pl.CostEstimate(
                flops=2 * length * feats * out_cols + 600_000_000,
                bytes_accessed=6_000_000,
                transcendentals=600_000,
            ),
            name="mix_rows",
        )(idx, sinks, proj, edge, taps, wout)

    sums = []
    for s in range(4):
        keep, send = mix(s)
        sums.append(added(keep, swapped(send)))
    opposite, following, before, own = sums
    up = ring(opposite[:half], "fs", 1)
    down = ring(opposite[half:], "fs", -1)
    up_b = ring(following[half:], "fs", 1)
    down_a = ring(before[:half], "fs", -1)
    up_a = ring(added(following[:half], up), "fs", 1)
    down_b = ring(added(before[half:], down), "fs", -1)
    top = added(own[:half], up_a, down_a)
    bottom = added(own[half:], up_b, down_b)
    return jnp.concatenate([top, bottom], 0)[None]


def solution(mesh):
    placed = (
        P(("grp", "fs"), ("sp", "tp"), None),
        P(),
        P(("sp", "fs"), "tp"),
        P(("sp", "fs"), "tp"),
        P(("sp", "fs"), "tp"),
        P(None, "tp"),
        P(("sp", "fs"), "tp"),
        P(("sp", "fs"), "tp"),
        P(("sp", "fs"), "tp"),
        P("tp"),
        P("tp", ("sp", "fs")),
        P("tp", ("sp", "fs")),
    )
    return jax.shard_map(
        local,
        mesh=mesh,
        in_specs=placed,
        out_specs=P(("grp", "fs"), ("sp", "tp"), None),
        check_vma=False,
    )
```

```python
import functools

import jax
import jax.numpy as jnp
from jax import lax
from jax.experimental import pallas as pl
from jax.experimental.pallas import tpu as pltpu
from jax.sharding import PartitionSpec as P


HEAD = 64
WINDOW = 128
TAPS = 3
EPSILON = 1e-06


ANY = pl.BlockSpec(memory_space=pl.ANY)
SMEM = pl.BlockSpec(memory_space=pltpu.SMEM)
VMEM = pl.BlockSpec(memory_space=pltpu.VMEM)


def ring(array, axis, by):
    size = lax.axis_size(axis)
    return lax.ppermute(array, axis, [(i, (i + by) % size) for i in range(size)])


def swapped(array):
    return lax.ppermute(array, "tp", [(0, 1), (1, 0)])


def gather_streams(streams, axis):
    size = lax.axis_size(axis)
    ahead, behind = list(streams), list(streams)
    pieces = [[s] for s in streams]
    spots = [0]
    for step in range(1, size // 2 + 1):
        last = step == size // 2
        spots += [size - step] if last else [size - step, step]
        for k in range(len(streams)):
            if not last or k % 2 == 1:
                ahead[k] = ring(ahead[k], axis, 1)
                pieces[k].append(ahead[k])
            if not last or k % 2 == 0:
                behind[k] = ring(behind[k], axis, -1)
                pieces[k].append(behind[k])
    return tuple(spots), pieces


def piece_copies(spots, refs, dst, src_cols, dst_cols, place, sems, first, block):
    copies = []
    for i, (offset, ref) in enumerate(zip(spots, refs)):
        row = pl.multiple_of(lax.rem(place + offset, len(spots)) * block, 128)
        copies.append(
            pltpu.make_async_copy(
                ref.at[:, src_cols], dst.at[pl.ds(row, block), dst_cols], sems.at[first + i]
            )
        )
    return copies


def edge_kernel(spots, block, feat, idx, *refs):
    count = len(spots)
    mine, theirs = refs[:4], refs[4:8]
    a_refs, b_refs = refs[8 : 8 + count], refs[8 + count : 8 + 2 * count]
    out, xs, wkv, wci, sems = refs[8 + 2 * count :]
    core, place = idx[0], idx[1]
    cols = wkv.shape[1]
    wide = wci.shape[1]
    copies = piece_copies(
        spots, a_refs, wkv, pl.ds(feat, cols), pl.ds(0, cols), place, sems, 4, block
    ) + piece_copies(
        spots, b_refs, wci, pl.ds(feat, wide), pl.ds(0, wide), place, sems, 4 + count, block
    )

    def rows_of(ref, s):
        start = ref.shape[0] - WINDOW
        return pltpu.make_async_copy(
            ref.at[pl.ds(start, WINDOW), :], xs.at[pl.ds(s * WINDOW, WINDOW), :], sems.at[s]
        )

    for c in copies:
        c.start()

    @pl.when(core == 1)
    def _():
        for s in range(4):
            rows_of(mine[s], s).start()

    @pl.when(core == 0)
    def _():
        for s in range(4):
            rows_of(theirs[s], s).start()

    for s in range(4):
        rows_of(mine[s], s).wait()
    for c in copies[:count]:
        c.wait()
    x = xs[...]
    kv = jnp.dot(x, wkv[...], preferred_element_type=jnp.float32).astype(jnp.bfloat16)
    for c in copies[count:]:
        c.wait()
    last = jnp.concatenate(
        [xs[(s + 1) * WINDOW - 16 : (s + 1) * WINDOW, :] for s in range(4)], axis=0
    )
    ci = jnp.dot(last, wci[...], preferred_element_type=jnp.float32).astype(jnp.bfloat16)
    ci = ci.astype(jnp.float32)
    gated = (ci[:, : wide // 2] * ci[:, wide // 2 :]).astype(jnp.bfloat16)
    for s in range(4):
        out[s, 0:WINDOW, :] = kv[s * WINDOW : (s + 1) * WINDOW]
        out[s, WINDOW : WINDOW + 16, :] = gated[s * 16 : (s + 1) * 16, :128]
        out[s, WINDOW + 16 : WINDOW + 32, :] = gated[s * 16 : (s + 1) * 16, 128:]


def project_kernel(spots, block, wide, idx, *refs):
    count = len(spots)
    mine, theirs = refs[:5], refs[5:10]
    a_refs, b_refs = refs[10 : 10 + count], refs[10 + count : 10 + 2 * count]
    out, wout, xs, ws, sems = refs[10 + 2 * count :]
    core, place = idx[0], idx[1]
    step = pl.program_id(0)
    half = xs.shape[1] // 2
    a_cols = ws.shape[1] - wide
    w_copies = piece_copies(
        spots, b_refs, ws, pl.ds(0, wide), pl.ds(0, wide), place, sems, 20, block
    ) + piece_copies(
        spots, a_refs, ws, pl.ds(0, a_cols), pl.ds(wide, a_cols), place, sems, 20 + count, block
    )
    o_copies = []
    parts = wout.shape[0] // block
    for i, (offset, ref) in enumerate(zip(spots, a_refs)):
        col = pl.multiple_of(lax.rem(place + offset, count) * block, 128)
        for j in range(parts):
            o_copies.append(
                pltpu.make_async_copy(
                    ref.at[:, pl.ds(a_cols + j * block, block)],
                    wout.at[pl.ds(j * block, block), pl.ds(col, block)],
                    sems.at[20 + 2 * count + parts * i + j],
                )
            )

    def x_copies(s):
        made = []
        for which, (group, base) in enumerate(
            ((mine, core * half), (theirs, (1 - core) * half))
        ):
            held = {0: (2,), 1: (3,), 2: (0, 1), 3: (4,)}[s]
            for j, g in enumerate(held):
                ref = group[g]
                row = pl.multiple_of(base + j * (half // 2), 128)
                made.append(
                    pltpu.make_async_copy(
                        ref, xs.at[s, pl.ds(row, ref.shape[0]), :], sems.at[4 * s + 2 * which + j]
                    )
                )
        return made

    @pl.when(step == 0)
    def _():
        for c in x_copies(0) + w_copies:
            c.start()
        for s in range(1, 4):
            for c in x_copies(s):
                c.start()
        for c in o_copies:
            c.start()
        for c in w_copies:
            c.wait()

    for s in range(4):

        @pl.when(step == s)
        def _():
            for c in x_copies(s):
                c.wait()
            if s == 3:
                for c in o_copies:
                    c.wait()

    acc = jnp.dot(xs[step], ws[...], preferred_element_type=jnp.float32)
    out[0] = acc.astype(jnp.bfloat16)


def mix_kernel(tasks, wide, idx, sinks, proj, edge, taps, wout, keep, send, acts, kt, vs):
    core, place = idx[0], idx[1]
    length = proj.shape[1]
    chans = wide // 3
    heads = chans // HEAD
    f32, bf16 = jnp.float32, jnp.bfloat16
    q_at, kv_at = wide, wide + chans
    pair = 2 * HEAD
    t = taps[...].astype(f32)

    def iota(shape, dim):
        return lax.broadcasted_iota(jnp.int32, shape, dim)

    pick_kt = (iota((chans, pair), 1) == jnp.bitwise_and(iota((chans, pair), 0), HEAD - 1)).astype(bf16)
    pick_v = (iota((pair, pair), 0) == jnp.bitwise_and(iota((pair, pair), 1), HEAD - 1) + HEAD).astype(bf16)
    row = iota((WINDOW, chans), 0)
    lane = iota((WINDOW, chans), 1)
    low = iota((WINDOW, pair), 1) < HEAD
    qi, ki = iota((WINDOW, 2 * WINDOW), 0), iota((WINDOW, 2 * WINDOW), 1)
    band = (ki > qi) & (ki <= qi + WINDOW)
    transposed = (((1,), (1,)), ((), ()))
    used = [0] * 2
    for i, (s, blocks) in enumerate(tasks):
        kv_before = edge[s, 0:WINDOW, :]
        kv_here = proj[s, :, kv_at : kv_at + pair]
        for at, kv in ((0, kv_before), (WINDOW, kv_here)):
            n = kv.shape[0]
            kt[i, :, at : at + n] = lax.dot_general(
                pick_kt, kv, transposed, preferred_element_type=f32
            ).astype(bf16)
            vs[i, at : at + n, 0:pair] = jnp.dot(kv, pick_v, preferred_element_type=f32).astype(bf16)
        vs[i, :, pair:] = jnp.ones((length + WINDOW, pair), bf16)

        def gated_rows(at, n):
            c = proj[s, at : at + n, chans : 2 * chans].astype(f32)
            return (c * proj[s, at : at + n, 2 * chans : 3 * chans].astype(f32)).astype(bf16).astype(f32)

        for n in blocks:
            at = n * WINDOW
            side = (2 * n * WINDOW) // length
            to = side * (length // 2) + used[side]
            used[side] += WINDOW
            if n == 0:
                tail = jnp.concatenate(
                    [edge[s, WINDOW : WINDOW + 16, :], edge[s, WINDOW + 16 : WINDOW + 32, :]], axis=1
                ).astype(f32)
            else:
                tail = gated_rows(at - 16, 16)
            before2, before1 = tail[14:15, :], tail[15:16, :]
            g = gated_rows(at, WINDOW)
            one = jnp.where(row == 0, before1, pltpu.roll(g, 1, 0))
            two = jnp.where(row == 0, before2, jnp.where(row == 1, before1, pltpu.roll(g, 2, 0)))
            convolved = two * t[0:1] + one * t[1:2] + g * t[2:3]
            out_gate = proj[s, at : at + WINDOW, 0:chans].astype(f32)
            acts[to : to + WINDOW, 0:chans] = (out_gate * convolved).astype(bf16)

            q = proj[s, at : at + WINDOW, q_at : q_at + chans]
            keys = kt[i, :, at : at + 2 * WINDOW]
            values = vs[i, at : at + 2 * WINDOW, :]
            allowed = band & ((ki >= WINDOW) | (place > 0)) if n == 0 else band
            outs = []
            for h in range(heads):
                qh = jnp.where((lane >= h * HEAD) & (lane < (h + 1) * HEAD), q, jnp.zeros_like(q))
                sc = jnp.dot(qh, keys, preferred_element_type=f32)
                sc = jnp.where(allowed, sc * (1.0 / 8.0), -jnp.inf)
                m = jnp.maximum(jnp.max(sc, axis=1, keepdims=True), sinks[h])
                e = jnp.exp(sc - m).astype(bf16)
                o = jnp.dot(e, values, preferred_element_type=f32)
                outs.append(o[:, :pair] / (o[:, pair:] + jnp.exp(sinks[h] - m)))
            for j in range(heads // 2):
                acts[to : to + WINDOW, chans + j * pair : chans + (j + 1) * pair] = jnp.where(
                    low, outs[2 * j], outs[2 * j + 1]
                ).astype(bf16)

    half = length // 2
    for dst, start in ((send, (1 - core) * half), (keep, core * half)):
        a = acts[pl.ds(pl.multiple_of(start, 128), half), :]
        dst[...] = jnp.dot(a, wout[...], preferred_element_type=f32).astype(bf16)


def added(*parts):
    total = parts[0].astype(jnp.float32)
    for p in parts[1:]:
        total = total + p.astype(jnp.float32)
    return total.astype(jnp.bfloat16)


def layer(
    tokens,
    norm_gain,
    w_bgate,
    w_cgate,
    w_conv_in,
    conv_taps,
    w_query,
    w_key,
    w_value,
    sink_logits,
    conv_out_weight,
    attn_out_weight,
):
    fs = lax.axis_size("fs")
    sp = lax.axis_size("sp")
    bf16, f32 = jnp.bfloat16, jnp.float32
    rows_in = w_bgate.shape[0]
    chans = w_bgate.shape[1] // fs
    kv_heads = w_key.shape[1] // HEAD
    block = rows_in * fs
    conv_t, attn_t = conv_out_weight.T, attn_out_weight.T
    packed = []
    for f in range(fs):
        cut = slice(f * chans, (f + 1) * chans)
        kv = f * kv_heads // fs
        kv_cut = slice(kv * HEAD, (kv + 1) * HEAD)
        packed.append(
            jnp.concatenate(
                [
                    w_query[:, cut],
                    w_key[:, kv_cut],
                    w_value[:, kv_cut],
                    conv_t[:, cut],
                    attn_t[:, cut],
                    w_bgate[:, cut],
                    w_cgate[:, cut],
                    w_conv_in[:, cut],
                ],
                axis=1,
            )
        )
    b_width, out_cols = 3 * chans, 2 * chans
    a_cols = chans + 2 * HEAD
    a_width = a_cols + out_cols
    in_cols = a_cols + b_width
    mine = lax.all_to_all(jnp.stack(packed), "fs", split_axis=0, concat_axis=0, tiled=True)
    mine = mine.reshape(block, a_width + b_width)
    out_part = mine[:, a_cols:a_width].reshape(block, out_cols // block, block)
    out_part = out_part.transpose(2, 1, 0).reshape(block, out_cols)
    stream_a = jnp.concatenate([mine[:, :a_cols], out_part], axis=1)
    stream_b = mine[:, a_width:]

    core, place, group = lax.axis_index("tp"), lax.axis_index("sp"), lax.axis_index("fs")
    idx = jnp.stack([core, place]).astype(jnp.int32)
    taps = lax.dynamic_slice_in_dim(conv_taps, group * chans, chans, 1)
    sinks = lax.dynamic_slice_in_dim(sink_logits, group * (chans // HEAD), chans // HEAD, 0)

    widened = tokens[0].astype(f32)
    normed = (
        widened
        * lax.rsqrt(jnp.mean(widened * widened, axis=-1, keepdims=True) + EPSILON)
        * norm_gain
    ).astype(bf16)
    normed, idx, taps, sinks = lax.optimization_barrier((normed, idx, taps, sinks))
    here, feats = normed.shape
    half = here // 2
    prev = ring(normed, "fs", 1)
    succ = ring(normed, "fs", -1)
    opp_a = ring(prev[:half], "fs", 1)
    opp_b = ring(succ[half:], "fs", -1)
    own_rows = [opp_a, opp_b, succ, prev, normed]
    other_rows = [swapped(a) for a in own_rows]

    spots, (blocks_b, blocks_a) = gather_streams([stream_b, stream_a], "sp")
    count = len(spots)
    length = 2 * here

    edge = pl.pallas_call(
        functools.partial(edge_kernel, spots, block, chans),
        out_shape=jax.ShapeDtypeStruct((4, WINDOW + 32, 2 * HEAD), bf16),
        in_specs=[SMEM] + [ANY] * (8 + 2 * count),
        out_specs=VMEM,
        scratch_shapes=[
            pltpu.VMEM((4 * WINDOW, feats), bf16),
            pltpu.VMEM((feats, 2 * HEAD), bf16),
            pltpu.VMEM((feats, 2 * chans), bf16),
            pltpu.SemaphoreType.DMA((4 + 2 * count,)),
        ],
        cost_estimate=pl.CostEstimate(flops=600_000_000, bytes_accessed=5_000_000, transcendentals=0),
        name="edge_rows",
    )(
        idx,
        *(group_rows[g] for group_rows in (own_rows, other_rows) for g in (2, 3, 1, 4)),
        *blocks_a,
        *blocks_b,
    )
    edge = lax.ppermute(edge, "sp", [(i, i + 1) for i in range(sp - 1)])

    proj, wout = pl.pallas_call(
        functools.partial(project_kernel, spots, block, b_width),
        out_shape=(
            jax.ShapeDtypeStruct((4, length, in_cols), bf16),
            jax.ShapeDtypeStruct((out_cols, feats), bf16),
        ),
        grid=(4,),
        in_specs=[SMEM] + [ANY] * (10 + 2 * count),
        out_specs=(
            pl.BlockSpec((1, length, in_cols), lambda s: (s, 0, 0)),
            pl.BlockSpec((out_cols, feats), lambda s: (0, 0)),
        ),
        scratch_shapes=[
            pltpu.VMEM((4, length, feats), bf16),
            pltpu.VMEM((feats, in_cols), bf16),
            pltpu.SemaphoreType.DMA((20 + (2 + out_cols // block) * count,)),
        ],
        cost_estimate=pl.CostEstimate(
            flops=2 * 4 * length * feats * in_cols, bytes_accessed=20_000_000, transcendentals=0
        ),
        compiler_params=pltpu.CompilerParams(dimension_semantics=("arbitrary",)),
        name="project_rows",
    )(idx, *own_rows, *other_rows, *blocks_a, *blocks_b)

    def mix(first, size, tasks):
        keep, send = pl.pallas_call(
            functools.partial(mix_kernel, tasks, b_width),
            out_shape=(jax.ShapeDtypeStruct((here, feats), bf16),) * 2,
            grid=(1,),
            in_specs=[
                SMEM,
                SMEM,
                pl.BlockSpec((size, length, in_cols), lambda i: (first, 0, 0)),
                pl.BlockSpec((size, WINDOW + 32, 2 * HEAD), lambda i: (first, 0, 0)),
                pl.BlockSpec((TAPS, chans), lambda i: (0, 0)),
                pl.BlockSpec((out_cols, feats), lambda i: (0, 0)),
            ],
            out_specs=(pl.BlockSpec((here, feats), lambda i: (0, 0)),) * 2,
            scratch_shapes=[
                pltpu.VMEM((length, out_cols), bf16),
                pltpu.VMEM((size, chans, length + WINDOW), bf16),
                pltpu.VMEM((size, length + WINDOW, 4 * HEAD), bf16),
            ],
            cost_estimate=pl.CostEstimate(
                flops=2 * length * feats * out_cols + 600_000_000,
                bytes_accessed=6_000_000,
                transcendentals=600_000,
            ),
        )(idx, sinks, proj, edge, taps, wout)
        return keep, swapped(send)

    def sent(array, by):
        return ring(array, "fs", by)

    keep, other = mix(2, 1, ((0, (0, 1, 2, 3)),))
    up = sent(added(keep[:half], other[:half]), 1)
    down = sent(added(keep[half:], other[half:]), -1)
    keep, other = mix(0, 2, ((0, (1, 3)), (1, (0, 2))))
    up_b = sent(added(keep[:half], other[:half]), 1)
    down_a = sent(added(keep[half:], other[half:]), -1)
    keep, other = mix(0, 2, ((0, (0, 2)), (1, (1, 3))))
    up_a = sent(added(keep[:half], other[:half], up), 1)
    down_b = sent(added(keep[half:], other[half:], down), -1)
    keep, other = mix(3, 1, ((0, (0, 1, 2, 3)),))
    top = added(keep[:half], other[:half], up_a, down_a)
    bottom = added(keep[half:], other[half:], up_b, down_b)
    return jnp.concatenate([top, bottom], 0)[None]


def solution(mesh):
    placed = (
        P(("grp", "fs"), ("sp", "tp"), None),
        P(),
        P(("sp", "fs"), "tp"),
        P(("sp", "fs"), "tp"),
        P(("sp", "fs"), "tp"),
        P(None, "tp"),
        P(("sp", "fs"), "tp"),
        P(("sp", "fs"), "tp"),
        P(("sp", "fs"), "tp"),
        P("tp"),
        P("tp", ("sp", "fs")),
        P("tp", ("sp", "fs")),
    )
    return jax.shard_map(
        layer,
        mesh=mesh,
        in_specs=placed,
        out_specs=P(("grp", "fs"), ("sp", "tp"), None),
        check_vma=False,
    )
```

```python
import functools

import jax
import jax.numpy as jnp
from jax import lax
from jax.experimental import pallas as pl
from jax.experimental.pallas import tpu as pltpu
from jax.sharding import PartitionSpec as P


HEAD = 64
WINDOW = 128
TAPS = 3
EPSILON = 1e-06


ANY = pl.BlockSpec(memory_space=pl.ANY)
SMEM = pl.BlockSpec(memory_space=pltpu.SMEM)
VMEM = pl.BlockSpec(memory_space=pltpu.VMEM)


def ring(array, axis, by):
    size = lax.axis_size(axis)
    return lax.ppermute(array, axis, [(i, (i + by) % size) for i in range(size)])


def swapped(array):
    return lax.ppermute(array, "tp", [(0, 1), (1, 0)])


def gather_streams(streams, axis):
    size = lax.axis_size(axis)
    ahead, behind = list(streams), list(streams)
    pieces = [[s] for s in streams]
    spots = [0]
    for step in range(1, size // 2 + 1):
        last = step == size // 2
        spots += [size - step] if last else [size - step, step]
        for k in range(len(streams)):
            if not last or k % 2 == 1:
                ahead[k] = ring(ahead[k], axis, 1)
                pieces[k].append(ahead[k])
            if not last or k % 2 == 0:
                behind[k] = ring(behind[k], axis, -1)
                pieces[k].append(behind[k])
    return tuple(spots), pieces


def piece_copies(spots, refs, dst, src_cols, dst_cols, place, sems, first, block):
    copies = []
    for i, (offset, ref) in enumerate(zip(spots, refs)):
        row = pl.multiple_of(lax.rem(place + offset, len(spots)) * block, 128)
        copies.append(
            pltpu.make_async_copy(
                ref.at[:, src_cols], dst.at[pl.ds(row, block), dst_cols], sems.at[first + i]
            )
        )
    return copies


def pack_kernel(wq, wk, wv, conv_t, attn_t, wb, wc, wi, out):
    fs = out.shape[0]
    chans = wq.shape[1] // fs
    for f in range(fs):
        cut = slice(f * chans, (f + 1) * chans)
        head = (f * wk.shape[1]) // (fs * HEAD) * HEAD
        kv = jnp.concatenate([wk[:, head : head + HEAD], wv[:, head : head + HEAD]], axis=1)
        at = 0
        for part in (wq[:, cut], kv, conv_t[:, cut], attn_t[:, cut], wb[:, cut], wc[:, cut], wi[:, cut]):
            out[f, :, at : at + part.shape[1]] = part
            at += part.shape[1]


def unpack_kernel(a_cols, mine, a, b):
    block, a_width = a.shape
    a[:, :a_cols] = mine[:, :a_cols]
    for at in range(a_cols, a_width, block):
        a[:, at : at + block] = mine[:, at : at + block].T
    b[...] = mine[:, a_width:]


def finish_kernel(keep, other, up_a, down_a, up_b, down_b, out):
    half = up_a.shape[0]
    for at, up, down in ((0, up_a, down_a), (half, up_b, down_b)):
        rows = slice(at, at + half)
        total = keep[rows, :].astype(jnp.float32) + other[rows, :].astype(jnp.float32)
        total = total + up[...].astype(jnp.float32) + down[...].astype(jnp.float32)
        out[rows, :] = total.astype(jnp.bfloat16)


def project_kernel(spots, block, wide, idx, *refs):
    count = len(spots)
    mine, theirs = refs[:5], refs[5:10]
    a_refs, b_refs = refs[10 : 10 + count], refs[10 + count : 10 + 2 * count]
    out, edge, wout, xs, ws, sems = refs[10 + 2 * count :]
    core, place = idx[0], idx[1]
    step = pl.program_id(0)
    half = xs.shape[1] // 2
    a_cols = ws.shape[1] - wide
    w_copies = piece_copies(
        spots, b_refs, ws, pl.ds(0, wide), pl.ds(0, wide), place, sems, 20, block
    ) + piece_copies(
        spots, a_refs, ws, pl.ds(0, a_cols), pl.ds(wide, a_cols), place, sems, 20 + count, block
    )
    o_copies = []
    parts = wout.shape[0] // block
    for i, (offset, ref) in enumerate(zip(spots, a_refs)):
        col = pl.multiple_of(lax.rem(place + offset, count) * block, 128)
        for j in range(parts):
            o_copies.append(
                pltpu.make_async_copy(
                    ref.at[:, pl.ds(a_cols + j * block, block)],
                    wout.at[pl.ds(j * block, block), pl.ds(col, block)],
                    sems.at[20 + 2 * count + parts * i + j],
                )
            )

    def x_copies(s):
        made = []
        for which, (group, base) in enumerate(
            ((mine, core * half), (theirs, (1 - core) * half))
        ):
            held = {0: (2,), 1: (3,), 2: (0, 1), 3: (4,)}[s]
            for j, g in enumerate(held):
                ref = group[g]
                row = pl.multiple_of(base + j * (half // 2), 128)
                made.append(
                    pltpu.make_async_copy(
                        ref, xs.at[s, pl.ds(row, ref.shape[0]), :], sems.at[4 * s + 2 * which + j]
                    )
                )
        return made

    @pl.when(step == 0)
    def _():
        for c in x_copies(0) + w_copies:
            c.start()
        for s in range(1, 4):
            for c in x_copies(s):
                c.start()
        for c in o_copies:
            c.start()
        for c in w_copies:
            c.wait()

    for s in range(4):

        @pl.when(step == s)
        def _():
            for c in x_copies(s):
                c.wait()
            if s == 3:
                for c in o_copies:
                    c.wait()

    acc = jnp.dot(xs[step], ws[...], preferred_element_type=jnp.float32)
    rounded = acc.astype(jnp.bfloat16)
    out[0] = rounded
    length, chans = xs.shape[1], wide // 3
    edge[0, 0:WINDOW, :] = rounded[length - WINDOW :, wide + chans :]
    last = rounded[length - 16 :, chans:wide].astype(jnp.float32)
    gated = (last[:, :chans] * last[:, chans:]).astype(jnp.bfloat16)
    edge[0, WINDOW : WINDOW + 16, :] = gated[:, : 2 * HEAD]
    edge[0, WINDOW + 16 : WINDOW + 32, :] = gated[:, 2 * HEAD :]


def mix_kernel(tasks, unroll, wide, idx, sinks, proj, edge, taps, wout, keep, send, acts, kt, vs):
    core, place = idx[0], idx[1]
    length = proj.shape[1]
    chans = wide // 3
    heads = chans // HEAD
    f32, bf16 = jnp.float32, jnp.bfloat16
    q_at, kv_at = wide, wide + chans
    pair = 2 * HEAD
    t = taps[...].astype(f32)

    def iota(shape, dim):
        return lax.broadcasted_iota(jnp.int32, shape, dim)

    pick_kt = (iota((chans, pair), 1) == jnp.bitwise_and(iota((chans, pair), 0), HEAD - 1)).astype(bf16)
    pick_v = (iota((pair, pair), 0) == jnp.bitwise_and(iota((pair, pair), 1), HEAD - 1) + HEAD).astype(bf16)
    row = iota((WINDOW, chans), 0)
    lane = iota((WINDOW, chans), 1)
    low = iota((WINDOW, pair), 1) < HEAD
    qi, ki = iota((WINDOW, 2 * WINDOW), 0), iota((WINDOW, 2 * WINDOW), 1)
    band = (ki > qi) & (ki <= qi + WINDOW)
    transposed = (((1,), (1,)), ((), ()))
    for i, (s, blocks) in enumerate(tasks):
        kv_before = edge[s, 0:WINDOW, :]
        kv_here = proj[s, :, kv_at : kv_at + pair]
        for at, kv in ((0, kv_before), (WINDOW, kv_here)):
            n = kv.shape[0]
            kt[i, :, at : at + n] = lax.dot_general(
                pick_kt, kv, transposed, preferred_element_type=f32
            ).astype(bf16)
            vs[i, at : at + n, 0:pair] = jnp.dot(kv, pick_v, preferred_element_type=f32).astype(bf16)
        vs[i, :, pair:] = jnp.ones((length + WINDOW, pair), bf16)

        def gated_rows(at, n, s=s):
            c = proj[s, pl.ds(at, n), chans : 2 * chans].astype(f32)
            return (c * proj[s, pl.ds(at, n), 2 * chans : 3 * chans].astype(f32)).astype(bf16).astype(f32)

        def one_block(n, to, s=s, i=i, gated_rows=gated_rows):
            at = pl.multiple_of(n * WINDOW, WINDOW)
            tail = gated_rows(pl.multiple_of(jnp.maximum(at - 16, 0), 16), 16)
            edge_tail = jnp.concatenate(
                [edge[s, WINDOW : WINDOW + 16, :], edge[s, WINDOW + 16 : WINDOW + 32, :]], axis=1
            ).astype(f32)
            tail = jnp.where(n == 0, edge_tail, tail)
            before2, before1 = tail[14:15, :], tail[15:16, :]
            g = gated_rows(at, WINDOW)
            one = jnp.where(row == 0, before1, pltpu.roll(g, 1, 0))
            two = jnp.where(row == 0, before2, jnp.where(row == 1, before1, pltpu.roll(g, 2, 0)))
            convolved = two * t[0:1] + one * t[1:2] + g * t[2:3]
            out_gate = proj[s, pl.ds(at, WINDOW), 0:chans].astype(f32)
            acts[pl.ds(to, WINDOW), 0:chans] = (out_gate * convolved).astype(bf16)

            q = proj[s, pl.ds(at, WINDOW), q_at : q_at + chans]
            keys = kt[i, :, pl.ds(at, 2 * WINDOW)]
            values = vs[i, pl.ds(at, 2 * WINDOW), :]
            allowed = band & ((ki >= WINDOW) | (place + n > 0))
            outs = []
            for h in range(heads):
                qh = jnp.where((lane >= h * HEAD) & (lane < (h + 1) * HEAD), q, jnp.zeros_like(q))
                sc = jnp.dot(qh, keys, preferred_element_type=f32)
                sc = jnp.where(allowed, sc * (1.0 / 8.0), -jnp.inf)
                m = jnp.maximum(jnp.max(sc, axis=1, keepdims=True), sinks[h])
                e = jnp.exp(sc - m).astype(bf16)
                o = jnp.dot(e, values, preferred_element_type=f32)
                outs.append(o[:, :pair] / (o[:, pair:] + jnp.exp(sinks[h] - m)))
            for j in range(heads // 2):
                acts[pl.ds(to, WINDOW), chans + j * pair : chans + (j + 1) * pair] = jnp.where(
                    low, outs[2 * j], outs[2 * j + 1]
                ).astype(bf16)

        first, stride = blocks
        steps = length // WINDOW // stride
        run = i * (length // 2) // len(tasks)

        def body(j, carry, s=s, i=i, first=first, stride=stride, run=run, one_block=one_block):
            n = first + j * stride
            each = length // 2 // WINDOW // stride
            to = (j // each) * (length // 2) + run + lax.rem(j, each) * WINDOW
            one_block(n, pl.multiple_of(to, WINDOW))
            return carry

        if unroll:
            for j in range(steps):
                body(jnp.int32(j), 0)
        else:
            lax.fori_loop(0, steps, body, 0)

    half = length // 2
    for dst, start in ((send, (1 - core) * half), (keep, core * half)):
        a = acts[pl.ds(pl.multiple_of(start, 128), half), :]
        if unroll:
            dst[...] = jnp.dot(a, wout[...], preferred_element_type=f32).astype(bf16)
            continue
        tile = 2 * WINDOW

        def columns(i, carry, a=a, dst=dst):
            cols = pl.ds(pl.multiple_of(i * tile, tile), tile)
            dst[:, cols] = jnp.dot(a, wout[:, cols], preferred_element_type=f32).astype(bf16)
            return carry

        lax.fori_loop(0, dst.shape[1] // tile, columns, 0)


def added(*parts):
    total = parts[0].astype(jnp.float32)
    for p in parts[1:]:
        total = total + p.astype(jnp.float32)
    return total.astype(jnp.bfloat16)


def layer(
    tokens,
    norm_gain,
    w_bgate,
    w_cgate,
    w_conv_in,
    conv_taps,
    w_query,
    w_key,
    w_value,
    sink_logits,
    conv_out_weight,
    attn_out_weight,
):
    fs = lax.axis_size("fs")
    sp = lax.axis_size("sp")
    bf16, f32 = jnp.bfloat16, jnp.float32
    rows_in = w_bgate.shape[0]
    chans = w_bgate.shape[1] // fs
    block = rows_in * fs
    b_width, out_cols = 3 * chans, 2 * chans
    a_cols = chans + 2 * HEAD
    a_width = a_cols + out_cols
    in_cols = a_cols + b_width
    packed = pl.pallas_call(
        pack_kernel,
        out_shape=jax.ShapeDtypeStruct((fs, rows_in, a_width + b_width), bf16),
        in_specs=[VMEM] * 8,
        out_specs=VMEM,
        name="pack_weights",
    )(w_query, w_key, w_value, conv_out_weight.T, attn_out_weight.T, w_bgate, w_cgate, w_conv_in)
    mine = lax.all_to_all(packed, "fs", split_axis=0, concat_axis=0, tiled=True)
    stream_a, stream_b = pl.pallas_call(
        functools.partial(unpack_kernel, a_cols),
        out_shape=(
            jax.ShapeDtypeStruct((block, a_width), bf16),
            jax.ShapeDtypeStruct((block, b_width), bf16),
        ),
        in_specs=[VMEM],
        out_specs=(VMEM, VMEM),
        name="unpack_weights",
    )(mine.reshape(block, a_width + b_width))

    core, place, group = lax.axis_index("tp"), lax.axis_index("sp"), lax.axis_index("fs")
    idx = jnp.stack([core, place]).astype(jnp.int32)
    taps = lax.dynamic_slice_in_dim(conv_taps, group * chans, chans, 1)
    sinks = lax.dynamic_slice_in_dim(sink_logits, group * (chans // HEAD), chans // HEAD, 0)

    widened = tokens[0].astype(f32)
    normed = (
        widened
        * lax.rsqrt(jnp.mean(widened * widened, axis=-1, keepdims=True) + EPSILON)
        * norm_gain
    ).astype(bf16)
    normed, idx, taps, sinks = lax.optimization_barrier((normed, idx, taps, sinks))
    here, feats = normed.shape
    half = here // 2
    prev = ring(normed, "fs", 1)
    succ = ring(normed, "fs", -1)
    opp_a = ring(prev[:half], "fs", 1)
    opp_b = ring(succ[half:], "fs", -1)
    own_rows = [opp_a, opp_b, succ, prev, normed]
    other_rows = [swapped(a) for a in own_rows]

    spots, (blocks_b, blocks_a) = gather_streams([stream_b, stream_a], "sp")
    count = len(spots)
    length = 2 * here

    proj, edge, wout = pl.pallas_call(
        functools.partial(project_kernel, spots, block, b_width),
        out_shape=(
            jax.ShapeDtypeStruct((4, length, in_cols), bf16),
            jax.ShapeDtypeStruct((4, WINDOW + 32, 2 * HEAD), bf16),
            jax.ShapeDtypeStruct((out_cols, feats), bf16),
        ),
        grid=(4,),
        in_specs=[SMEM] + [ANY] * (10 + 2 * count),
        out_specs=(
            pl.BlockSpec((1, length, in_cols), lambda s: (s, 0, 0)),
            pl.BlockSpec((1, WINDOW + 32, 2 * HEAD), lambda s: (s, 0, 0)),
            pl.BlockSpec((out_cols, feats), lambda s: (0, 0)),
        ),
        scratch_shapes=[
            pltpu.VMEM((4, length, feats), bf16),
            pltpu.VMEM((feats, in_cols), bf16),
            pltpu.SemaphoreType.DMA((20 + (2 + out_cols // block) * count,)),
        ],
        cost_estimate=pl.CostEstimate(
            flops=2 * 4 * length * feats * in_cols, bytes_accessed=20_000_000, transcendentals=0
        ),
        compiler_params=pltpu.CompilerParams(dimension_semantics=("arbitrary",)),
        name="project_rows",
    )(idx, *own_rows, *other_rows, *blocks_a, *blocks_b)
    edge = lax.ppermute(edge, "sp", [(i, i + 1) for i in range(sp - 1)])

    def mix(name, first, size, tasks):
        keep, send = pl.pallas_call(
            functools.partial(mix_kernel, tasks, name == "opp", b_width),
            out_shape=(jax.ShapeDtypeStruct((here, feats), bf16),) * 2,
            grid=(1,),
            in_specs=[
                SMEM,
                SMEM,
                pl.BlockSpec((size, length, in_cols), lambda i: (first, 0, 0)),
                pl.BlockSpec((size, WINDOW + 32, 2 * HEAD), lambda i: (first, 0, 0)),
                pl.BlockSpec((TAPS, chans), lambda i: (0, 0)),
                pl.BlockSpec((out_cols, feats), lambda i: (0, 0)),
            ],
            out_specs=(pl.BlockSpec((here, feats), lambda i: (0, 0)),) * 2,
            scratch_shapes=[
                pltpu.VMEM((length, out_cols), bf16),
                pltpu.VMEM((size, chans, length + WINDOW), bf16),
                pltpu.VMEM((size, length + WINDOW, 4 * HEAD), bf16),
            ],
            cost_estimate=pl.CostEstimate(
                flops=2 * length * feats * out_cols + 600_000_000,
                bytes_accessed=6_000_000,
                transcendentals=600_000,
            ),
        )(idx, sinks, proj, edge, taps, wout)
        return keep, swapped(send)

    def sent(array, by):
        return ring(array, "fs", by)

    keep, other = mix("opp", 2, 1, ((0, (0, 1)),))
    up = sent(added(keep[:half], other[:half]), 1)
    down = sent(added(keep[half:], other[half:]), -1)
    keep, other = mix("x", 0, 2, ((0, (1, 2)), (1, (0, 2))))
    up_b = sent(added(keep[:half], other[:half]), 1)
    down_a = sent(added(keep[half:], other[half:]), -1)
    keep, other = mix("y", 0, 2, ((0, (0, 2)), (1, (1, 2))))
    up_a = sent(added(keep[:half], other[:half], up), 1)
    down_b = sent(added(keep[half:], other[half:], down), -1)
    keep, other = mix("own", 3, 1, ((0, (0, 1)),))
    out = pl.pallas_call(
        finish_kernel,
        out_shape=jax.ShapeDtypeStruct((here, feats), bf16),
        in_specs=[VMEM] * 6,
        out_specs=VMEM,
        name="finish_rows",
    )(keep, other, up_a, down_a, up_b, down_b)
    return out[None]


def solution(mesh):
    placed = (
        P(("grp", "fs"), ("sp", "tp"), None),
        P(),
        P(("sp", "fs"), "tp"),
        P(("sp", "fs"), "tp"),
        P(("sp", "fs"), "tp"),
        P(None, "tp"),
        P(("sp", "fs"), "tp"),
        P(("sp", "fs"), "tp"),
        P(("sp", "fs"), "tp"),
        P("tp"),
        P("tp", ("sp", "fs")),
        P("tp", ("sp", "fs")),
    )
    return jax.shard_map(
        layer,
        mesh=mesh,
        in_specs=placed,
        out_specs=P(("grp", "fs"), ("sp", "tp"), None),
        check_vma=False,
    )
```

```python
import functools

import jax
import jax.numpy as jnp
from jax import lax
from jax.experimental import pallas as pl
from jax.experimental.pallas import tpu as pltpu
from jax.sharding import PartitionSpec as P


HEAD = 64
WINDOW = 128
TAPS = 3
EPSILON = 1e-06


ANY = pl.BlockSpec(memory_space=pl.ANY)
SMEM = pl.BlockSpec(memory_space=pltpu.SMEM)
VMEM = pl.BlockSpec(memory_space=pltpu.VMEM)


def ring(array, axis, by):
    size = lax.axis_size(axis)
    return lax.ppermute(array, axis, [(i, (i + by) % size) for i in range(size)])


def pack_kernel(wq, wk, wv, conv_t, attn_t, wb, wc, wi, out):
    fs = out.shape[0]
    chans = wq.shape[1] // fs
    for f in range(fs):
        cut = slice(f * chans, (f + 1) * chans)
        head = (f * wk.shape[1]) // (fs * HEAD) * HEAD
        kv = jnp.concatenate([wk[:, head : head + HEAD], wv[:, head : head + HEAD]], axis=1)
        at = 0
        for part in (wb[:, cut], wc[:, cut], wi[:, cut], wq[:, cut], kv, conv_t[:, cut], attn_t[:, cut]):
            out[f, :, at : at + part.shape[1]] = part
            at += part.shape[1]


def turn_kernel(in_cols, mine, out):
    block, width = out.shape
    out[:, :in_cols] = mine[:, :in_cols]
    for at in range(in_cols, width, block):
        out[:, at : at + block] = mine[:, at : at + block].T


def finish_kernel(low, high, up_a, down_a, up_b, down_b, out):
    half = up_a.shape[0]
    for at, own, up, down in ((0, low, up_a, down_a), (half, high, up_b, down_b)):
        total = own[...].astype(jnp.float32) + up[...].astype(jnp.float32)
        total = total + down[...].astype(jnp.float32)
        out[at : at + half, :] = total.astype(jnp.bfloat16)


def project_kernel(wide, weights, *refs):
    opp_a, opp_b, succ, prev, own, out, edge, wout, xs, ws, sems = refs
    step = pl.program_id(0)
    half = opp_a.shape[0]
    block = weights.shape[2]
    blocks = weights.shape[0]
    in_cols = ws.shape[3]
    parts = (weights.shape[3] - in_cols) // block
    bf16, f32 = jnp.bfloat16, jnp.float32
    x_copies = [
        pltpu.make_async_copy(ref, xs.at[s, pl.ds(at, ref.shape[0]), :], sems.at[i])
        for i, (ref, s, at) in enumerate(
            ((succ, 0, 0), (prev, 1, 0), (opp_a, 2, 0), (opp_b, 2, half), (own, 3, 0))
        )
    ]
    w_copies = [
        pltpu.make_async_copy(weights.at[:, t, :, pl.ds(0, in_cols)], ws.at[t], sems.at[5 + t])
        for t in range(2)
    ]

    def out_copies(t):
        return [
            pltpu.make_async_copy(
                weights.at[j, t, :, pl.ds(in_cols + b * block, block)],
                wout.at[pl.ds((t * parts + b) * block, block), pl.ds(j * block, block)],
                sems.at[7 + (t * parts + b) * blocks + j],
            )
            for b in range(parts)
            for j in range(blocks)
        ]

    @pl.when(step == 0)
    def _():
        for c in x_copies + w_copies:
            c.start()
        for c in out_copies(0):
            c.start()
        for c in x_copies:
            c.wait()
        w_copies[0].wait()

    @pl.when(step == 1)
    def _():
        for c in out_copies(1):
            c.start()
        w_copies[1].wait()

    seqs, length, feats = xs.shape
    x = xs[...].reshape(seqs * length, feats)
    w = ws[step].reshape(feats, in_cols)
    rounded = jnp.dot(x, w, preferred_element_type=f32).astype(bf16).reshape(seqs, length, in_cols)
    out[0] = rounded
    chans = wide // 3
    for s in range(seqs):
        edge[0, s, 0:WINDOW, :] = rounded[s, length - WINDOW :, wide + chans :]
        last = rounded[s, length - 16 :, chans:wide].astype(f32)
        gated = (last[:, :chans] * last[:, chans:]).astype(bf16)
        edge[0, s, WINDOW : WINDOW + 16, :] = gated[:, : 2 * HEAD]
        edge[0, s, WINDOW + 16 : WINDOW + 32, :] = gated[:, 2 * HEAD :]

    @pl.when(step == 1)
    def _():
        for t in range(2):
            for c in out_copies(t):
                c.wait()


def mix_kernel(tasks, wide, idx, sinks, proj, edge, taps, wout, low, high, acts):
    place = idx[0]
    chans = wide // 3
    heads = chans // HEAD
    f32, bf16 = jnp.float32, jnp.bfloat16
    q_at, kv_at = wide, wide + chans
    pair = 2 * HEAD

    def iota(shape, dim):
        return lax.broadcasted_iota(jnp.int32, shape, dim)

    pick_kt = (iota((chans, pair), 1) == jnp.bitwise_and(iota((chans, pair), 0), HEAD - 1)).astype(bf16)
    pick_v = (iota((pair, pair), 0) == jnp.bitwise_and(iota((pair, pair), 1), HEAD - 1) + HEAD).astype(bf16)
    row = iota((WINDOW, chans), 0)
    lane = iota((WINDOW, chans), 1)
    left = iota((WINDOW, pair), 1) < HEAD
    qi, ki = iota((WINDOW, 2 * WINDOW), 0), iota((WINDOW, 2 * WINDOW), 1)
    band = (ki > qi) & (ki <= qi + WINDOW)
    first = band & ((ki >= WINDOW) | (place > 0))
    ones = jnp.ones((2 * WINDOW, pair), bf16)
    transposed = (((1,), (1,)), ((), ()))
    for slot, (s, n) in enumerate(tasks):
        at, to = n * WINDOW, slot * WINDOW
        for side in range(2):

            def gated_rows(start, rows):
                c = proj[side, s, start : start + rows, chans : 2 * chans].astype(f32)
                i = proj[side, s, start : start + rows, 2 * chans : 3 * chans].astype(f32)
                return (c * i).astype(bf16).astype(f32)

            t = taps[side]
            base = side * 2 * chans
            if n == 0:
                tail = jnp.concatenate(
                    [edge[side, s, WINDOW : WINDOW + 16, :], edge[side, s, WINDOW + 16 : WINDOW + 32, :]],
                    axis=1,
                ).astype(f32)
            else:
                tail = gated_rows(at - 16, 16)
            before2, before1 = tail[14:15, :], tail[15:16, :]
            g = gated_rows(at, WINDOW)
            one = jnp.where(row == 0, before1, pltpu.roll(g, 1, 0))
            two = jnp.where(row == 0, before2, jnp.where(row == 1, before1, pltpu.roll(g, 2, 0)))
            convolved = two * t[0:1] + one * t[1:2] + g * t[2:3]
            out_gate = proj[side, s, at : at + WINDOW, 0:chans].astype(f32)
            acts[to : to + WINDOW, base : base + chans] = (out_gate * convolved).astype(bf16)

            kv_here = proj[side, s, at : at + WINDOW, kv_at : kv_at + pair]
            if n == 0:
                kv_before = edge[side, s, 0:WINDOW, :]
            else:
                kv_before = proj[side, s, at - WINDOW : at, kv_at : kv_at + pair]
            kv = jnp.concatenate([kv_before, kv_here], axis=0)
            keys = lax.dot_general(pick_kt, kv, transposed, preferred_element_type=f32).astype(bf16)
            values = jnp.dot(kv, pick_v, preferred_element_type=f32).astype(bf16)
            values = jnp.concatenate([values, ones], axis=1)
            q = proj[side, s, at : at + WINDOW, q_at : q_at + chans]
            allowed = first if n == 0 else band
            outs = []
            for h in range(heads):
                qh = jnp.where((lane >= h * HEAD) & (lane < (h + 1) * HEAD), q, jnp.zeros_like(q))
                sc = jnp.dot(qh, keys, preferred_element_type=f32)
                sc = jnp.where(allowed, sc * (1.0 / 8.0), -jnp.inf)
                sink = sinks[side, h]
                m = jnp.maximum(jnp.max(sc, axis=1, keepdims=True), sink)
                e = jnp.exp(sc - m).astype(bf16)
                o = jnp.dot(e, values, preferred_element_type=f32)
                outs.append(o[:, :pair] / (o[:, pair:] + jnp.exp(sink - m)))
            for j in range(heads // 2):
                col = base + chans + j * pair
                acts[to : to + WINDOW, col : col + pair] = jnp.where(
                    left, outs[2 * j], outs[2 * j + 1]
                ).astype(bf16)

    product = jnp.dot(acts[...], wout[...], preferred_element_type=f32).astype(bf16)
    low[...] = product[:WINDOW]
    high[...] = product[WINDOW:]


def added(*parts):
    total = parts[0].astype(jnp.float32)
    for p in parts[1:]:
        total = total + p.astype(jnp.float32)
    return total.astype(jnp.bfloat16)


def layer(
    tokens,
    norm_gain,
    w_bgate,
    w_cgate,
    w_conv_in,
    conv_taps,
    w_query,
    w_key,
    w_value,
    sink_logits,
    conv_out_weight,
    attn_out_weight,
):
    fs = lax.axis_size("fs")
    sp = lax.axis_size("sp")
    tp = lax.axis_size("tp")
    bf16, f32 = jnp.bfloat16, jnp.float32
    rows_in = w_bgate.shape[0]
    chans = w_bgate.shape[1] // fs
    block = rows_in * fs
    b_width, out_cols = 3 * chans, 2 * chans
    in_cols = b_width + chans + 2 * HEAD
    width = in_cols + out_cols
    packed = pl.pallas_call(
        pack_kernel,
        out_shape=jax.ShapeDtypeStruct((fs, rows_in, width), bf16),
        in_specs=[VMEM] * 8,
        out_specs=VMEM,
        name="pack_weights",
    )(w_query, w_key, w_value, conv_out_weight.T, attn_out_weight.T, w_bgate, w_cgate, w_conv_in)
    mine = lax.all_to_all(packed, "fs", split_axis=0, concat_axis=0, tiled=True)
    mine = pl.pallas_call(
        functools.partial(turn_kernel, in_cols),
        out_shape=jax.ShapeDtypeStruct((block, width), bf16),
        in_specs=[VMEM],
        out_specs=VMEM,
        name="turn_weights",
    )(mine.reshape(block, width))
    weights = lax.all_gather(mine, ("sp", "tp"), axis=0, tiled=True)
    weights = weights.reshape(sp, tp, block, width)

    core, place, group = lax.axis_index("tp"), lax.axis_index("sp"), lax.axis_index("fs")
    heads = chans // HEAD
    idx = jnp.stack([place * tp + core, place]).astype(jnp.int32)
    taps = lax.dynamic_slice_in_dim(conv_taps, group * chans, chans, 1).astype(f32)
    sinks = lax.dynamic_slice_in_dim(sink_logits, group * heads, heads, 0)
    small = jnp.concatenate([taps, jnp.pad(sinks[None], ((0, 0), (0, chans - heads)))], axis=0)

    widened = tokens[0].astype(f32)
    normed = (
        widened
        * lax.rsqrt(jnp.mean(widened * widened, axis=-1, keepdims=True) + EPSILON)
        * norm_gain
    ).astype(bf16)
    here, feats = normed.shape
    half = here // 2
    prev = ring(normed, "fs", 1)
    succ = ring(normed, "fs", -1)
    opp_a = ring(prev[:half], "fs", 1)
    opp_b = ring(succ[half:], "fs", -1)
    theirs = lax.ppermute(small, "tp", [(0, 1), (1, 0)])
    both = jnp.where(core == 0, jnp.stack([small, theirs]), jnp.stack([theirs, small]))
    taps, sinks = both[:, :TAPS], both[:, TAPS, :heads]

    squares = out_cols // block
    proj, edge, wout = pl.pallas_call(
        functools.partial(project_kernel, b_width),
        out_shape=(
            jax.ShapeDtypeStruct((tp, fs, here, in_cols), bf16),
            jax.ShapeDtypeStruct((tp, fs, WINDOW + 32, 2 * HEAD), bf16),
            jax.ShapeDtypeStruct((tp * out_cols, feats), bf16),
        ),
        grid=(tp,),
        in_specs=[ANY] * 6,
        out_specs=(
            pl.BlockSpec((1, fs, here, in_cols), lambda t: (t, 0, 0, 0)),
            pl.BlockSpec((1, fs, WINDOW + 32, 2 * HEAD), lambda t: (t, 0, 0, 0)),
            pl.BlockSpec((tp * out_cols, feats), lambda t: (0, 0)),
        ),
        scratch_shapes=[
            pltpu.VMEM((fs, here, feats), bf16),
            pltpu.VMEM((tp, sp, block, in_cols), bf16),
            pltpu.SemaphoreType.DMA((7 + tp * squares * sp,)),
        ],
        cost_estimate=pl.CostEstimate(
            flops=2 * tp * fs * here * feats * in_cols, bytes_accessed=25_000_000, transcendentals=0
        ),
        compiler_params=pltpu.CompilerParams(dimension_semantics=("arbitrary",)),
        name="project_rows",
    )(weights, opp_a, opp_b, succ, prev, normed)
    edge = lax.ppermute(edge, ("sp", "tp"), [(i, i + 1) for i in range(sp * tp - 1)])

    def mix(first, size, tasks):
        return pl.pallas_call(
            functools.partial(mix_kernel, tasks, b_width),
            out_shape=(jax.ShapeDtypeStruct((half, feats), bf16),) * 2,
            grid=(1,),
            in_specs=[
                SMEM,
                SMEM,
                pl.BlockSpec((tp, size, here, in_cols), lambda i: (0, first, 0, 0)),
                pl.BlockSpec((tp, size, WINDOW + 32, 2 * HEAD), lambda i: (0, first, 0, 0)),
                pl.BlockSpec((tp, TAPS, chans), lambda i: (0, 0, 0)),
                pl.BlockSpec((tp * out_cols, feats), lambda i: (0, 0)),
            ],
            out_specs=(pl.BlockSpec((half, feats), lambda i: (0, 0)),) * 2,
            scratch_shapes=[pltpu.VMEM((here, tp * out_cols), bf16)],
            cost_estimate=pl.CostEstimate(
                flops=2 * here * feats * tp * out_cols + 600_000_000,
                bytes_accessed=8_000_000,
                transcendentals=600_000,
            ),
        )(idx, sinks, proj, edge, taps, wout)

    def sent(array, by):
        return ring(array, "fs", by)

    low, high = mix(2, 1, ((0, 0), (0, 1)))
    up, down = sent(low, 1), sent(high, -1)
    low, high = mix(0, 2, ((0, 1), (1, 0)))
    up_b, down_a = sent(low, 1), sent(high, -1)
    low, high = mix(0, 2, ((0, 0), (1, 1)))
    up_a, down_b = sent(added(low, up), 1), sent(added(high, down), -1)
    low, high = mix(3, 1, ((0, 0), (0, 1)))
    out = pl.pallas_call(
        finish_kernel,
        out_shape=jax.ShapeDtypeStruct((here, feats), bf16),
        in_specs=[VMEM] * 6,
        out_specs=VMEM,
        name="finish_rows",
    )(low, high, up_a, down_a, up_b, down_b)
    return out[None]


def solution(mesh):
    placed = (
        P(("grp", "fs"), ("sp", "tp"), None),
        P(),
        P(("sp", "fs"), "tp"),
        P(("sp", "fs"), "tp"),
        P(("sp", "fs"), "tp"),
        P(None, "tp"),
        P(("sp", "fs"), "tp"),
        P(("sp", "fs"), "tp"),
        P(("sp", "fs"), "tp"),
        P("tp"),
        P("tp", ("sp", "fs")),
        P("tp", ("sp", "fs")),
    )
    return jax.shard_map(
        layer,
        mesh=mesh,
        in_specs=placed,
        out_specs=P(("grp", "fs"), ("sp", "tp"), None),
        check_vma=False,
    )
```

```python
import functools

import jax
import jax.numpy as jnp
from jax import lax
from jax.experimental import pallas as pl
from jax.experimental.pallas import tpu as pltpu
from jax.sharding import PartitionSpec as P


HEAD = 64
WINDOW = 128
TAPS = 3
EPSILON = 1e-06


ANY = pl.BlockSpec(memory_space=pl.ANY)
SMEM = pl.BlockSpec(memory_space=pltpu.SMEM)
VMEM = pl.BlockSpec(memory_space=pltpu.VMEM)


def ring(array, axis, by):
    size = lax.axis_size(axis)
    return lax.ppermute(array, axis, [(i, (i + by) % size) for i in range(size)])


def pack_kernel(wq, wk, wv, conv_t, attn_t, wb, wc, wi, out):
    fs = out.shape[0]
    chans = wq.shape[1] // fs
    for f in range(fs):
        cut = slice(f * chans, (f + 1) * chans)
        head = (f * wk.shape[1]) // (fs * HEAD) * HEAD
        kv = jnp.concatenate([wk[:, head : head + HEAD], wv[:, head : head + HEAD]], axis=1)
        at = 0
        for part in (wb[:, cut], wc[:, cut], wi[:, cut], wq[:, cut], kv, conv_t[:, cut], attn_t[:, cut]):
            out[f, :, at : at + part.shape[1]] = part
            at += part.shape[1]


def turn_kernel(in_cols, mine, out):
    block, width = out.shape
    out[:, :in_cols] = mine[:, :in_cols]
    for at in range(in_cols, width, block):
        out[:, at : at + block] = mine[:, at : at + block].T


def finish_kernel(low, high, up_a, down_a, up_b, down_b, out):
    half = up_a.shape[0]
    for at, own, up, down in ((0, low, up_a, down_a), (half, high, up_b, down_b)):
        total = own[...].astype(jnp.float32) + up[...].astype(jnp.float32)
        total = total + down[...].astype(jnp.float32)
        out[at : at + half, :] = total.astype(jnp.bfloat16)


def project_kernel(wide, weights, *refs):
    opp_a, opp_b, succ, prev, own, out, edge, wout, xs, ws, wo, sems = refs
    step = pl.program_id(0)
    half = opp_a.shape[0]
    block = weights.shape[2]
    blocks = weights.shape[0]
    in_cols = ws.shape[3]
    parts = (weights.shape[3] - in_cols) // block
    bf16, f32 = jnp.bfloat16, jnp.float32
    x_copies = [
        pltpu.make_async_copy(ref, xs.at[s, pl.ds(at, ref.shape[0]), :], sems.at[i])
        for i, (ref, s, at) in enumerate(
            ((succ, 0, 0), (prev, 1, 0), (opp_a, 2, 0), (opp_b, 2, half), (own, 3, 0))
        )
    ]
    w_copies = [
        pltpu.make_async_copy(weights.at[:, t, :, pl.ds(0, in_cols)], ws.at[t], sems.at[5 + t])
        for t in range(2)
    ]

    def out_copies(t):
        return [
            pltpu.make_async_copy(
                weights.at[j, t, :, pl.ds(in_cols + b * block, block)],
                wo.at[pl.ds((t * parts + b) * block, block), pl.ds(j * block, block)],
                sems.at[7 + (t * parts + b) * blocks + j],
            )
            for b in range(parts)
            for j in range(blocks)
        ]

    laid_out = pltpu.make_async_copy(wo, wout, sems.at[7 + 2 * parts * blocks])

    @pl.when(step == 0)
    def _():
        for c in x_copies + w_copies[:1]:
            c.start()
        for c in x_copies + w_copies[:1]:
            c.wait()
        w_copies[1].start()
        for t in range(2):
            for c in out_copies(t):
                c.start()

    @pl.when(step == 1)
    def _():
        w_copies[1].wait()
        for t in range(2):
            for c in out_copies(t):
                c.wait()
        laid_out.start()

    seqs, length, feats = xs.shape
    x = xs[...].reshape(seqs * length, feats)
    w = ws[step].reshape(feats, in_cols)
    rounded = jnp.dot(x, w, preferred_element_type=f32).astype(bf16).reshape(seqs, length, in_cols)
    out[0] = rounded
    chans = wide // 3
    for s in range(seqs):
        edge[0, s, 0:WINDOW, :] = rounded[s, length - WINDOW :, wide + chans :]
        last = rounded[s, length - 16 :, chans:wide].astype(f32)
        gated = (last[:, :chans] * last[:, chans:]).astype(bf16)
        edge[0, s, WINDOW : WINDOW + 16, :] = gated[:, : 2 * HEAD]
        edge[0, s, WINDOW + 16 : WINDOW + 32, :] = gated[:, 2 * HEAD :]

    @pl.when(step == 1)
    def _():
        laid_out.wait()


def mix_kernel(blocks, wide, idx, sinks, taps, wout, *refs):
    projs, edges = refs[:2], refs[2:-3]
    low, high, acts = refs[-3:]
    place = idx[0]
    chans = wide // 3
    heads = chans // HEAD
    f32, bf16 = jnp.float32, jnp.bfloat16
    q_at, kv_at = wide, wide + chans
    pair = 2 * HEAD

    def iota(shape, dim):
        return lax.broadcasted_iota(jnp.int32, shape, dim)

    pick_kt = (iota((chans, pair), 1) == jnp.bitwise_and(iota((chans, pair), 0), HEAD - 1)).astype(bf16)
    pick_v = (iota((pair, pair), 0) == jnp.bitwise_and(iota((pair, pair), 1), HEAD - 1) + HEAD).astype(bf16)
    row = iota((WINDOW, chans), 0)
    lane = iota((WINDOW, chans), 1)
    left = iota((WINDOW, pair), 1) < HEAD
    qi, ki = iota((WINDOW, 2 * WINDOW), 0), iota((WINDOW, 2 * WINDOW), 1)
    band = (ki > qi) & (ki <= qi + WINDOW)
    first = band & ((ki >= WINDOW) | (place > 0))
    ones = jnp.ones((2 * WINDOW, pair), bf16)
    transposed = (((1,), (1,)), ((), ()))
    for slot, n in enumerate(blocks):
        at, to = n * WINDOW, slot * WINDOW
        proj, edge = projs[slot], edges[slot] if n == 0 else None
        for side in range(2):

            def gated_rows(start, rows):
                c = proj[side, 0, start : start + rows, chans : 2 * chans].astype(f32)
                i = proj[side, 0, start : start + rows, 2 * chans : 3 * chans].astype(f32)
                return (c * i).astype(bf16).astype(f32)

            t = taps[side]
            base = side * 2 * chans
            if n == 0:
                tail = jnp.concatenate(
                    [edge[side, 0, WINDOW : WINDOW + 16, :], edge[side, 0, WINDOW + 16 : WINDOW + 32, :]],
                    axis=1,
                ).astype(f32)
            else:
                tail = gated_rows(at - 16, 16)
            before2, before1 = tail[14:15, :], tail[15:16, :]
            g = gated_rows(at, WINDOW)
            one = jnp.where(row == 0, before1, pltpu.roll(g, 1, 0))
            two = jnp.where(row == 0, before2, jnp.where(row == 1, before1, pltpu.roll(g, 2, 0)))
            convolved = two * t[0:1] + one * t[1:2] + g * t[2:3]
            out_gate = proj[side, 0, at : at + WINDOW, 0:chans].astype(f32)
            acts[to : to + WINDOW, base : base + chans] = (out_gate * convolved).astype(bf16)

            kv_here = proj[side, 0, at : at + WINDOW, kv_at : kv_at + pair]
            if n == 0:
                kv_before = edge[side, 0, 0:WINDOW, :]
            else:
                kv_before = proj[side, 0, at - WINDOW : at, kv_at : kv_at + pair]
            kv = jnp.concatenate([kv_before, kv_here], axis=0)
            keys = lax.dot_general(pick_kt, kv, transposed, preferred_element_type=f32).astype(bf16)
            values = jnp.dot(kv, pick_v, preferred_element_type=f32).astype(bf16)
            values = jnp.concatenate([values, ones], axis=1)
            q = proj[side, 0, at : at + WINDOW, q_at : q_at + chans]
            allowed = first if n == 0 else band
            outs = []
            for h in range(heads):
                qh = jnp.where((lane >= h * HEAD) & (lane < (h + 1) * HEAD), q, jnp.zeros_like(q))
                sc = jnp.dot(qh, keys, preferred_element_type=f32)
                sc = jnp.where(allowed, sc * (1.0 / 8.0), -jnp.inf)
                sink = sinks[side, h]
                m = jnp.maximum(jnp.max(sc, axis=1, keepdims=True), sink)
                e = jnp.exp(sc - m).astype(bf16)
                o = jnp.dot(e, values, preferred_element_type=f32)
                outs.append(o[:, :pair] / (o[:, pair:] + jnp.exp(sink - m)))
            for j in range(heads // 2):
                col = base + chans + j * pair
                acts[to : to + WINDOW, col : col + pair] = jnp.where(
                    left, outs[2 * j], outs[2 * j + 1]
                ).astype(bf16)

    product = jnp.dot(acts[...], wout[...], preferred_element_type=f32).astype(bf16)
    low[...] = product[:WINDOW]
    high[...] = product[WINDOW:]


def added(*parts):
    total = parts[0].astype(jnp.float32)
    for p in parts[1:]:
        total = total + p.astype(jnp.float32)
    return total.astype(jnp.bfloat16)


def layer(
    tokens,
    norm_gain,
    w_bgate,
    w_cgate,
    w_conv_in,
    conv_taps,
    w_query,
    w_key,
    w_value,
    sink_logits,
    conv_out_weight,
    attn_out_weight,
):
    fs = lax.axis_size("fs")
    sp = lax.axis_size("sp")
    tp = lax.axis_size("tp")
    bf16, f32 = jnp.bfloat16, jnp.float32
    rows_in = w_bgate.shape[0]
    chans = w_bgate.shape[1] // fs
    block = rows_in * fs
    b_width, out_cols = 3 * chans, 2 * chans
    in_cols = b_width + chans + 2 * HEAD
    width = in_cols + out_cols
    packed = pl.pallas_call(
        pack_kernel,
        out_shape=jax.ShapeDtypeStruct((fs, rows_in, width), bf16),
        in_specs=[VMEM] * 8,
        out_specs=VMEM,
        name="pack_weights",
    )(w_query, w_key, w_value, conv_out_weight.T, attn_out_weight.T, w_bgate, w_cgate, w_conv_in)
    mine = lax.all_to_all(packed, "fs", split_axis=0, concat_axis=0, tiled=True)
    mine = pl.pallas_call(
        functools.partial(turn_kernel, in_cols),
        out_shape=jax.ShapeDtypeStruct((block, width), bf16),
        in_specs=[VMEM],
        out_specs=VMEM,
        name="turn_weights",
    )(mine.reshape(block, width))
    weights = lax.all_gather(mine, ("sp", "tp"), axis=0, tiled=True)
    weights = weights.reshape(sp, tp, block, width)

    core, place, group = lax.axis_index("tp"), lax.axis_index("sp"), lax.axis_index("fs")
    heads = chans // HEAD
    idx = jnp.stack([place * tp + core, place]).astype(jnp.int32)
    taps = lax.dynamic_slice_in_dim(conv_taps, group * chans, chans, 1).astype(f32)
    sinks = lax.dynamic_slice_in_dim(sink_logits, group * heads, heads, 0)
    small = jnp.concatenate([taps, jnp.pad(sinks[None], ((0, 0), (0, chans - heads)))], axis=0)

    widened = tokens[0].astype(f32)
    normed = (
        widened
        * lax.rsqrt(jnp.mean(widened * widened, axis=-1, keepdims=True) + EPSILON)
        * norm_gain
    ).astype(bf16)
    here, feats = normed.shape
    half = here // 2
    prev = ring(normed, "fs", 1)
    succ = ring(normed, "fs", -1)
    opp_a = ring(prev[:half], "fs", 1)
    opp_b = ring(succ[half:], "fs", -1)
    theirs = lax.ppermute(small, "tp", [(0, 1), (1, 0)])
    both = jnp.where(core == 0, jnp.stack([small, theirs]), jnp.stack([theirs, small]))
    taps, sinks = both[:, :TAPS], both[:, TAPS, :heads]
    weights, idx, taps, sinks = lax.optimization_barrier((weights, idx, taps, sinks))

    squares = out_cols // block
    proj, edge, wout = pl.pallas_call(
        functools.partial(project_kernel, b_width),
        out_shape=(
            jax.ShapeDtypeStruct((tp, fs, here, in_cols), bf16),
            jax.ShapeDtypeStruct((tp, fs, WINDOW + 32, 2 * HEAD), bf16),
            jax.ShapeDtypeStruct((tp * out_cols, feats), bf16),
        ),
        grid=(tp,),
        in_specs=[ANY] * 6,
        out_specs=(
            pl.BlockSpec((1, fs, here, in_cols), lambda t: (t, 0, 0, 0)),
            pl.BlockSpec((1, fs, WINDOW + 32, 2 * HEAD), lambda t: (t, 0, 0, 0)),
            ANY,
        ),
        scratch_shapes=[
            pltpu.VMEM((fs, here, feats), bf16),
            pltpu.VMEM((tp, sp, block, in_cols), bf16),
            pltpu.VMEM((tp * out_cols, feats), bf16),
            pltpu.SemaphoreType.DMA((8 + tp * squares * sp,)),
        ],
        cost_estimate=pl.CostEstimate(
            flops=2 * tp * fs * here * feats * in_cols, bytes_accessed=25_000_000, transcendentals=0
        ),
        compiler_params=pltpu.CompilerParams(dimension_semantics=("arbitrary",)),
        name="project_rows",
    )(weights, opp_a, opp_b, succ, prev, normed)
    edge = lax.ppermute(edge, ("sp", "tp"), [(i, i + 1) for i in range(sp * tp - 1)])

    def mix(tasks):
        seqs, blocks = zip(*tasks)
        edged = [q for q, n in tasks if n == 0]

        def part(shape, q):
            return pl.BlockSpec((tp, 1) + shape, lambda i, q=q: (0, q, 0, 0))

        return pl.pallas_call(
            functools.partial(mix_kernel, blocks, b_width),
            out_shape=(jax.ShapeDtypeStruct((half, feats), bf16),) * 2,
            grid=(1,),
            in_specs=[
                SMEM,
                SMEM,
                pl.BlockSpec((tp, TAPS, chans), lambda i: (0, 0, 0)),
                pl.BlockSpec((tp * out_cols, feats), lambda i: (0, 0)),
            ]
            + [part((here, in_cols), q) for q in seqs]
            + [part((WINDOW + 32, 2 * HEAD), q) for q in (seqs if edged else ())],
            out_specs=(pl.BlockSpec((half, feats), lambda i: (0, 0)),) * 2,
            scratch_shapes=[pltpu.VMEM((here, tp * out_cols), bf16)],
            cost_estimate=pl.CostEstimate(
                flops=2 * here * feats * tp * out_cols + 600_000_000,
                bytes_accessed=8_000_000,
                transcendentals=600_000,
            ),
        )(idx, sinks, taps, wout, proj, proj, *((edge, edge) if edged else ()))

    def sent(array, by):
        return ring(array, "fs", by)

    succ_q, prev_q, opp_q, own_q = range(4)
    low, high = mix(((succ_q, 1), (opp_q, 1)))
    down, up_b = sent(high, -1), sent(low, 1)
    low, high = mix(((opp_q, 0), (prev_q, 0)))
    up, down_a = sent(low, 1), sent(high, -1)
    low, high = mix(((succ_q, 0), (prev_q, 1)))
    down_b, up_a = sent(added(high, down), -1), sent(added(low, up), 1)
    low, high = mix(((own_q, 0), (own_q, 1)))
    out = pl.pallas_call(
        finish_kernel,
        out_shape=jax.ShapeDtypeStruct((here, feats), bf16),
        in_specs=[VMEM] * 6,
        out_specs=VMEM,
        name="finish_rows",
    )(low, high, up_a, down_a, up_b, down_b)
    return out[None]


def solution(mesh):
    placed = (
        P(("grp", "fs"), ("sp", "tp"), None),
        P(),
        P(("sp", "fs"), "tp"),
        P(("sp", "fs"), "tp"),
        P(("sp", "fs"), "tp"),
        P(None, "tp"),
        P(("sp", "fs"), "tp"),
        P(("sp", "fs"), "tp"),
        P(("sp", "fs"), "tp"),
        P("tp"),
        P("tp", ("sp", "fs")),
        P("tp", ("sp", "fs")),
    )
    return jax.shard_map(
        layer,
        mesh=mesh,
        in_specs=placed,
        out_specs=P(("grp", "fs"), ("sp", "tp"), None),
        check_vma=False,
    )
```

```python
import functools

import jax
import jax.numpy as jnp
from jax import lax
from jax.experimental import pallas as pl
from jax.experimental.pallas import tpu as pltpu
from jax.sharding import PartitionSpec as P


HEAD = 64
WINDOW = 128
TAPS = 3
EPSILON = 1e-06


ANY = pl.BlockSpec(memory_space=pl.ANY)
SMEM = pl.BlockSpec(memory_space=pltpu.SMEM)
VMEM = pl.BlockSpec(memory_space=pltpu.VMEM)


def ring(array, axis, by):
    size = lax.axis_size(axis)
    return lax.ppermute(array, axis, [(i, (i + by) % size) for i in range(size)])


def pack_kernel(wq, wk, wv, conv_t, attn_t, wb, wc, wi, out):
    fs = out.shape[0]
    chans = wq.shape[1] // fs
    for f in range(fs):
        cut = slice(f * chans, (f + 1) * chans)
        head = (f * wk.shape[1]) // (fs * HEAD) * HEAD
        kv = jnp.concatenate([wk[:, head : head + HEAD], wv[:, head : head + HEAD]], axis=1)
        at = 0
        for part in (wb[:, cut], wc[:, cut], wi[:, cut], wq[:, cut], kv, conv_t[:, cut], attn_t[:, cut]):
            out[f, :, at : at + part.shape[1]] = part
            at += part.shape[1]


def turn_kernel(in_cols, mine, out):
    block, width = out.shape
    out[:, :in_cols] = mine[:, :in_cols]
    for at in range(in_cols, width, block):
        out[:, at : at + block] = mine[:, at : at + block].T


def project_kernel(wide, weights, *refs):
    opp_a, opp_b, succ, prev, own, out, edge, wout, xs, ws, wo, sems = refs
    step = pl.program_id(0)
    half = opp_a.shape[0]
    block = weights.shape[2]
    blocks = weights.shape[0]
    in_cols = ws.shape[3]
    parts = (weights.shape[3] - in_cols) // block
    bf16, f32 = jnp.bfloat16, jnp.float32
    x_copies = [
        pltpu.make_async_copy(ref, xs.at[s, pl.ds(at, ref.shape[0]), :], sems.at[i])
        for i, (ref, s, at) in enumerate(
            ((succ, 0, 0), (prev, 1, 0), (opp_a, 2, 0), (opp_b, 2, half), (own, 3, 0))
        )
    ]
    cuts = ((0, 4 * block), (4 * block, in_cols - 4 * block))

    def w_copy(t, k):
        cols = pl.ds(*cuts[k])
        return pltpu.make_async_copy(weights.at[:, t, :, cols], ws.at[t, :, :, cols], sems.at[5 + 2 * t + k])

    def out_copies(t):
        return [
            pltpu.make_async_copy(
                weights.at[j, t, :, pl.ds(in_cols + b * block, block)],
                wo.at[pl.ds((t * parts + b) * block, block), pl.ds(j * block, block)],
                sems.at[9 + (t * parts + b) * blocks + j],
            )
            for b in range(parts)
            for j in range(blocks)
        ]

    laid_out = pltpu.make_async_copy(wo, wout, sems.at[9 + 2 * parts * blocks])

    @pl.when(step == 0)
    def _():
        for c in x_copies:
            c.start()
        w_copy(0, 0).start()
        w_copy(0, 1).start()
        for c in x_copies:
            c.wait()
        w_copy(0, 0).wait()

    @pl.when(step == 1)
    def _():
        w_copy(1, 0).wait()
        w_copy(1, 1).wait()
        for t in range(2):
            for c in out_copies(t):
                c.wait()
        laid_out.start()

    seqs, length, feats = xs.shape
    x = xs[...].reshape(seqs * length, feats)

    def project(k):
        cols = slice(cuts[k][0], cuts[k][0] + cuts[k][1])
        w = ws[step, :, :, cols].reshape(feats, cuts[k][1])
        product = jnp.dot(x, w, preferred_element_type=f32).astype(bf16)
        out[0, :, :, cols] = product.reshape(seqs, length, cuts[k][1])

    project(0)

    @pl.when(step == 0)
    def _():
        w_copy(0, 1).wait()
        w_copy(1, 0).start()
        w_copy(1, 1).start()
        for t in range(2):
            for c in out_copies(t):
                c.start()

    project(1)
    chans = wide // 3
    for s in range(seqs):
        edge[0, s, 0:WINDOW, :] = out[0, s, length - WINDOW :, wide + chans :]
        last = out[0, s, length - 16 :, chans:wide].astype(f32)
        gated = (last[:, :chans] * last[:, chans:]).astype(bf16)
        edge[0, s, WINDOW : WINDOW + 16, :] = gated[:, : 2 * HEAD]
        edge[0, s, WINDOW + 16 : WINDOW + 32, :] = gated[:, 2 * HEAD :]

    @pl.when(step == 1)
    def _():
        laid_out.wait()


def mix_kernel(blocks, pieces, wide, idx, sinks, taps, wout, *refs):
    acts, wo, sem = refs[-3:]
    outs_at = len(refs) - 3 - len(pieces)
    results = refs[outs_at:-3]
    first_edge = 2 if 0 in blocks else 0
    projs, edges = refs[:2], refs[2 : 2 + first_edge]
    arrived = refs[2 + first_edge : outs_at]
    wanted = pltpu.make_async_copy(wout, wo, sem)
    wanted.start()
    place = idx[0]
    chans = wide // 3
    heads = chans // HEAD
    f32, bf16 = jnp.float32, jnp.bfloat16
    q_at, kv_at = wide, wide + chans
    pair = 2 * HEAD

    def iota(shape, dim):
        return lax.broadcasted_iota(jnp.int32, shape, dim)

    pick_kt = (iota((chans, pair), 1) == jnp.bitwise_and(iota((chans, pair), 0), HEAD - 1)).astype(bf16)
    pick_v = (iota((pair, pair), 0) == jnp.bitwise_and(iota((pair, pair), 1), HEAD - 1) + HEAD).astype(bf16)
    row = iota((WINDOW, chans), 0)
    lane = iota((WINDOW, chans), 1)
    left = iota((WINDOW, pair), 1) < HEAD
    qi, ki = iota((WINDOW, 2 * WINDOW), 0), iota((WINDOW, 2 * WINDOW), 1)
    band = (ki > qi) & (ki <= qi + WINDOW)
    first = band & ((ki >= WINDOW) | (place > 0))
    ones = jnp.ones((2 * WINDOW, pair), bf16)
    transposed = (((1,), (1,)), ((), ()))
    for slot, n in enumerate(blocks):
        at, to = n * WINDOW, slot * WINDOW
        proj, edge = projs[slot], edges[slot] if n == 0 else None
        for side in range(2):

            def gated_rows(start, rows):
                c = proj[side, 0, start : start + rows, chans : 2 * chans].astype(f32)
                i = proj[side, 0, start : start + rows, 2 * chans : 3 * chans].astype(f32)
                return (c * i).astype(bf16).astype(f32)

            t = taps[side]
            base = side * 2 * chans
            if n == 0:
                tail = jnp.concatenate(
                    [edge[side, 0, WINDOW : WINDOW + 16, :], edge[side, 0, WINDOW + 16 : WINDOW + 32, :]],
                    axis=1,
                ).astype(f32)
            else:
                tail = gated_rows(at - 16, 16)
            before2, before1 = tail[14:15, :], tail[15:16, :]
            g = gated_rows(at, WINDOW)
            one = jnp.where(row == 0, before1, pltpu.roll(g, 1, 0))
            two = jnp.where(row == 0, before2, jnp.where(row == 1, before1, pltpu.roll(g, 2, 0)))
            convolved = two * t[0:1] + one * t[1:2] + g * t[2:3]
            out_gate = proj[side, 0, at : at + WINDOW, 0:chans].astype(f32)
            acts[to : to + WINDOW, base : base + chans] = (out_gate * convolved).astype(bf16)

            kv_here = proj[side, 0, at : at + WINDOW, kv_at : kv_at + pair]
            if n == 0:
                kv_before = edge[side, 0, 0:WINDOW, :]
            else:
                kv_before = proj[side, 0, at - WINDOW : at, kv_at : kv_at + pair]
            kv = jnp.concatenate([kv_before, kv_here], axis=0)
            keys = lax.dot_general(pick_kt, kv, transposed, preferred_element_type=f32).astype(bf16)
            values = jnp.dot(kv, pick_v, preferred_element_type=f32).astype(bf16)
            values = jnp.concatenate([values, ones], axis=1)
            q = proj[side, 0, at : at + WINDOW, q_at : q_at + chans]
            allowed = first if n == 0 else band
            outs = []
            for h in range(heads):
                qh = jnp.where((lane >= h * HEAD) & (lane < (h + 1) * HEAD), q, jnp.zeros_like(q))
                sc = jnp.dot(qh, keys, preferred_element_type=f32)
                sc = jnp.where(allowed, sc * (1.0 / 8.0), -jnp.inf)
                sink = sinks[side, h]
                m = jnp.maximum(jnp.max(sc, axis=1, keepdims=True), sink)
                e = jnp.exp(sc - m).astype(bf16)
                o = jnp.dot(e, values, preferred_element_type=f32)
                outs.append(o[:, :pair] / (o[:, pair:] + jnp.exp(sink - m)))
            for j in range(heads // 2):
                col = base + chans + j * pair
                acts[to : to + WINDOW, col : col + pair] = jnp.where(
                    left, outs[2 * j], outs[2 * j + 1]
                ).astype(bf16)

    wanted.wait()
    product = jnp.dot(acts[...], wo[...], preferred_element_type=f32)
    if arrived:
        product = product + jnp.concatenate([a[...] for a in arrived], axis=0).astype(f32)
    product = product.astype(bf16)
    at = 0
    for ref in results:
        ref[...] = product[at : at + ref.shape[0]]
        at += ref.shape[0]


def added(*parts):
    total = parts[0].astype(jnp.float32)
    for p in parts[1:]:
        total = total + p.astype(jnp.float32)
    return total.astype(jnp.bfloat16)


def layer(
    tokens,
    norm_gain,
    w_bgate,
    w_cgate,
    w_conv_in,
    conv_taps,
    w_query,
    w_key,
    w_value,
    sink_logits,
    conv_out_weight,
    attn_out_weight,
):
    fs = lax.axis_size("fs")
    sp = lax.axis_size("sp")
    tp = lax.axis_size("tp")
    bf16, f32 = jnp.bfloat16, jnp.float32
    rows_in = w_bgate.shape[0]
    chans = w_bgate.shape[1] // fs
    block = rows_in * fs
    b_width, out_cols = 3 * chans, 2 * chans
    in_cols = b_width + chans + 2 * HEAD
    width = in_cols + out_cols
    packed = pl.pallas_call(
        pack_kernel,
        out_shape=jax.ShapeDtypeStruct((fs, rows_in, width), bf16),
        in_specs=[VMEM] * 8,
        out_specs=VMEM,
        name="pack_weights",
    )(w_query, w_key, w_value, conv_out_weight.T, attn_out_weight.T, w_bgate, w_cgate, w_conv_in)
    mine = lax.all_to_all(packed, "fs", split_axis=0, concat_axis=0, tiled=True)
    mine = pl.pallas_call(
        functools.partial(turn_kernel, in_cols),
        out_shape=jax.ShapeDtypeStruct((block, width), bf16),
        in_specs=[VMEM],
        out_specs=VMEM,
        name="turn_weights",
    )(mine.reshape(block, width))
    weights = lax.all_gather(mine, ("sp", "tp"), axis=0, tiled=True)
    weights = weights.reshape(sp, tp, block, width)

    core, place, group = lax.axis_index("tp"), lax.axis_index("sp"), lax.axis_index("fs")
    heads = chans // HEAD
    idx = jnp.stack([place * tp + core, place]).astype(jnp.int32)
    taps = lax.dynamic_slice_in_dim(conv_taps, group * chans, chans, 1).astype(f32)
    sinks = lax.dynamic_slice_in_dim(sink_logits, group * heads, heads, 0)
    small = jnp.concatenate([taps, jnp.pad(sinks[None], ((0, 0), (0, chans - heads)))], axis=0)

    widened = tokens[0].astype(f32)
    normed = (
        widened
        * lax.rsqrt(jnp.mean(widened * widened, axis=-1, keepdims=True) + EPSILON)
        * norm_gain
    ).astype(bf16)
    here, feats = normed.shape
    half = here // 2
    prev = ring(normed, "fs", 1)
    succ = ring(normed, "fs", -1)
    opp_a = ring(prev[:half], "fs", 1)
    opp_b = ring(succ[half:], "fs", -1)
    theirs = lax.ppermute(small, "tp", [(0, 1), (1, 0)])
    both = jnp.where(core == 0, jnp.stack([small, theirs]), jnp.stack([theirs, small]))
    taps, sinks = both[:, :TAPS], both[:, TAPS, :heads]
    weights, idx, taps, sinks = lax.optimization_barrier((weights, idx, taps, sinks))

    squares = out_cols // block
    proj, edge, wout = pl.pallas_call(
        functools.partial(project_kernel, b_width),
        out_shape=(
            jax.ShapeDtypeStruct((tp, fs, here, in_cols), bf16),
            jax.ShapeDtypeStruct((tp, fs, WINDOW + 32, 2 * HEAD), bf16),
            jax.ShapeDtypeStruct((tp * out_cols, feats), bf16),
        ),
        grid=(tp,),
        in_specs=[ANY] * 6,
        out_specs=(
            pl.BlockSpec((1, fs, here, in_cols), lambda t: (t, 0, 0, 0)),
            pl.BlockSpec((1, fs, WINDOW + 32, 2 * HEAD), lambda t: (t, 0, 0, 0)),
            ANY,
        ),
        scratch_shapes=[
            pltpu.VMEM((fs, here, feats), bf16),
            pltpu.VMEM((tp, sp, block, in_cols), bf16),
            pltpu.VMEM((tp * out_cols, feats), bf16),
            pltpu.SemaphoreType.DMA((10 + tp * squares * sp,)),
        ],
        cost_estimate=pl.CostEstimate(
            flops=2 * tp * fs * here * feats * in_cols, bytes_accessed=25_000_000, transcendentals=0
        ),
        compiler_params=pltpu.CompilerParams(dimension_semantics=("arbitrary",)),
        name="project_rows",
    )(weights, opp_a, opp_b, succ, prev, normed)
    edge = lax.ppermute(edge, ("sp", "tp"), [(i, i + 1) for i in range(sp * tp - 1)])

    def mix(tasks, pieces, arrived=()):
        seqs, blocks = zip(*tasks)
        edged = [q for q, n in tasks if n == 0]

        def part(shape, q):
            return pl.BlockSpec((tp, 1) + shape, lambda i, q=q: (0, q, 0, 0))

        return pl.pallas_call(
            functools.partial(mix_kernel, blocks, pieces, b_width),
            out_shape=tuple(jax.ShapeDtypeStruct((n, feats), bf16) for n in pieces),
            grid=(1,),
            in_specs=[SMEM, SMEM, pl.BlockSpec((tp, TAPS, chans), lambda i: (0, 0, 0)), ANY]
            + [part((here, in_cols), q) for q in seqs]
            + [part((WINDOW + 32, 2 * HEAD), q) for q in (seqs if edged else ())]
            + [pl.BlockSpec(a.shape, lambda i: (0, 0)) for a in arrived],
            out_specs=tuple(pl.BlockSpec((n, feats), lambda i: (0, 0)) for n in pieces),
            scratch_shapes=[
                pltpu.VMEM((here, tp * out_cols), bf16),
                pltpu.VMEM((tp * out_cols, feats), bf16),
                pltpu.SemaphoreType.DMA,
            ],
            cost_estimate=pl.CostEstimate(
                flops=2 * here * feats * tp * out_cols + 600_000_000,
                bytes_accessed=8_000_000,
                transcendentals=600_000,
            ),
        )(idx, sinks, taps, wout, proj, proj, *((edge, edge) if edged else ()), *arrived)

    def sent(array, by):
        return ring(array, "fs", by)

    succ_q, prev_q, opp_q, own_q = range(4)
    low, high = mix(((succ_q, 1), (opp_q, 1)), (half, half))
    down, up_b = sent(high, -1), sent(low, 1)
    quarter = half // 2
    low_1, low_2, high = mix(((opp_q, 0), (prev_q, 0)), (quarter, quarter, half))
    up_1, up_2 = sent(low_1, 1), sent(low_2, 1)
    down_a = sent(high, -1)
    low_1, low_2, high = mix(((succ_q, 0), (prev_q, 1)), (quarter, quarter, half))
    down_b = sent(added(high, down), -1)
    up_a1, up_a2 = sent(added(low_1, up_1), 1), sent(added(low_2, up_2), 1)
    (own,) = mix(((own_q, 0), (own_q, 1)), (here,), (down_a, up_b))
    return added(own, jnp.concatenate([up_a1, up_a2, down_b], 0))[None]


def solution(mesh):
    placed = (
        P(("grp", "fs"), ("sp", "tp"), None),
        P(),
        P(("sp", "fs"), "tp"),
        P(("sp", "fs"), "tp"),
        P(("sp", "fs"), "tp"),
        P(None, "tp"),
        P(("sp", "fs"), "tp"),
        P(("sp", "fs"), "tp"),
        P(("sp", "fs"), "tp"),
        P("tp"),
        P("tp", ("sp", "fs")),
        P("tp", ("sp", "fs")),
    )
    return jax.shard_map(
        layer,
        mesh=mesh,
        in_specs=placed,
        out_specs=P(("grp", "fs"), ("sp", "tp"), None),
        check_vma=False,
    )
```

```python
import functools

import jax
import jax.numpy as jnp
from jax import lax
from jax.experimental import pallas as pl
from jax.experimental.pallas import tpu as pltpu
from jax.sharding import PartitionSpec as P


HEAD = 64
WINDOW = 128
TAPS = 3
EPSILON = 1e-06


ANY = pl.BlockSpec(memory_space=pl.ANY)
SMEM = pl.BlockSpec(memory_space=pltpu.SMEM)
VMEM = pl.BlockSpec(memory_space=pltpu.VMEM)


def ring(array, axis, by):
    size = lax.axis_size(axis)
    return lax.ppermute(array, axis, [(i, (i + by) % size) for i in range(size)])


def pack_kernel(wq, wk, wv, conv_t, attn_t, wb, wc, wi, out):
    fs = out.shape[0]
    chans = wq.shape[1] // fs
    for f in range(fs):
        cut = slice(f * chans, (f + 1) * chans)
        head = (f * wk.shape[1]) // (fs * HEAD) * HEAD
        kv = jnp.concatenate([wk[:, head : head + HEAD], wv[:, head : head + HEAD]], axis=1)
        at = 0
        for part in (wb[:, cut], wc[:, cut], wi[:, cut], wq[:, cut], kv, conv_t[:, cut], attn_t[:, cut]):
            out[f, :, at : at + part.shape[1]] = part
            at += part.shape[1]


def turn_kernel(in_cols, mine, out):
    block, width = out.shape
    out[:, :in_cols] = mine[:, :in_cols]
    for at in range(in_cols, width, block):
        out[:, at : at + block] = mine[:, at : at + block].T


def project_kernel(wide, weights, *refs):
    opp_a, opp_b, succ, prev, own, out, kvs, edge, wout, xs, ws, wkv, wo, sems = refs
    step = pl.program_id(0)
    half = opp_a.shape[0]
    block = weights.shape[2]
    blocks = weights.shape[0]
    main = ws.shape[3]
    pair = wkv.shape[2] // 2
    parts = (weights.shape[3] - main - pair) // block
    bf16, f32 = jnp.bfloat16, jnp.float32
    x_copies = [
        pltpu.make_async_copy(ref, xs.at[s, pl.ds(at, ref.shape[0]), :], sems.at[i])
        for i, (ref, s, at) in enumerate(
            ((succ, 0, 0), (prev, 1, 0), (opp_a, 2, 0), (opp_b, 2, half), (own, 3, 0))
        )
    ]
    w_copies = [
        pltpu.make_async_copy(weights.at[:, t, :, pl.ds(0, main)], ws.at[t], sems.at[5 + t])
        for t in range(2)
    ]
    kv_copies = [
        pltpu.make_async_copy(
            weights.at[:, t, :, pl.ds(main, pair)], wkv.at[:, :, pl.ds(t * pair, pair)], sems.at[7 + t]
        )
        for t in range(2)
    ]
    out_copies = [
        pltpu.make_async_copy(
            weights.at[j, t, :, pl.ds(main + pair + b * block, block)],
            wo.at[pl.ds((t * parts + b) * block, block), pl.ds(j * block, block)],
            sems.at[9 + (t * parts + b) * blocks + j],
        )
        for t in range(2)
        for b in range(parts)
        for j in range(blocks)
    ]
    laid_out = pltpu.make_async_copy(wo, wout, sems.at[9 + 2 * parts * blocks])

    @pl.when(step == 0)
    def _():
        for c in x_copies + w_copies[:1]:
            c.start()
        for c in x_copies + w_copies[:1]:
            c.wait()
        for c in w_copies[1:] + kv_copies + out_copies:
            c.start()

    @pl.when(step == 1)
    def _():
        for c in w_copies[1:] + kv_copies + out_copies:
            c.wait()
        laid_out.start()

    seqs, length, feats = xs.shape
    x = xs[...].reshape(seqs * length, feats)
    w = ws[step].reshape(feats, main)
    rounded = jnp.dot(x, w, preferred_element_type=f32).astype(bf16).reshape(seqs, length, main)
    out[0] = rounded
    chans = wide // 3
    for s in range(seqs):
        last = rounded[s, length - 16 :, chans:wide].astype(f32)
        gated = (last[:, :chans] * last[:, chans:]).astype(bf16)
        edge[step, s, WINDOW : WINDOW + 16, :] = gated[:, : 2 * HEAD]
        edge[step, s, WINDOW + 16 : WINDOW + 32, :] = gated[:, 2 * HEAD :]

    @pl.when(step == 1)
    def _():
        k = wkv[...].reshape(feats, 2 * pair)
        both = jnp.dot(x, k, preferred_element_type=f32).astype(bf16).reshape(seqs, length, 2 * pair)
        kvs[...] = both
        for t in range(2):
            for s in range(seqs):
                edge[t, s, 0:WINDOW, :] = both[s, length - WINDOW :, t * pair : (t + 1) * pair]
        laid_out.wait()


def mix_kernel(blocks, pieces, wide, idx, sinks, taps, wout, *refs):
    acts, wo, sem = refs[-3:]
    outs_at = len(refs) - 3 - len(pieces)
    results = refs[outs_at:-3]
    has_edge = 2 if 0 in blocks else 0
    projs, kvs, edges = refs[:2], refs[2:4], refs[4 : 4 + has_edge]
    arrived = refs[4 + has_edge : outs_at]
    wanted = pltpu.make_async_copy(wout, wo, sem)
    wanted.start()
    place = idx[0]
    chans = wide // 3
    heads = chans // HEAD
    f32, bf16 = jnp.float32, jnp.bfloat16
    q_at = wide
    pair = 2 * HEAD

    def iota(shape, dim):
        return lax.broadcasted_iota(jnp.int32, shape, dim)

    pick_kt = (iota((chans, pair), 1) == jnp.bitwise_and(iota((chans, pair), 0), HEAD - 1)).astype(bf16)
    pick_v = (iota((pair, pair), 0) == jnp.bitwise_and(iota((pair, pair), 1), HEAD - 1) + HEAD).astype(bf16)
    row = iota((WINDOW, chans), 0)
    lane = iota((WINDOW, chans), 1)
    left = iota((WINDOW, pair), 1) < HEAD
    qi, ki = iota((WINDOW, 2 * WINDOW), 0), iota((WINDOW, 2 * WINDOW), 1)
    band = (ki > qi) & (ki <= qi + WINDOW)
    first = band & ((ki >= WINDOW) | (place > 0))
    ones = jnp.ones((2 * WINDOW, pair), bf16)
    transposed = (((1,), (1,)), ((), ()))
    for slot, n in enumerate(blocks):
        at, to = n * WINDOW, slot * WINDOW
        proj, kv_rows, edge = projs[slot], kvs[slot], edges[slot] if n == 0 else None
        for side in range(2):

            def gated_rows(start, rows):
                c = proj[side, 0, start : start + rows, chans : 2 * chans].astype(f32)
                i = proj[side, 0, start : start + rows, 2 * chans : 3 * chans].astype(f32)
                return (c * i).astype(bf16).astype(f32)

            t = taps[side]
            base = side * 2 * chans
            if n == 0:
                tail = jnp.concatenate(
                    [edge[side, 0, WINDOW : WINDOW + 16, :], edge[side, 0, WINDOW + 16 : WINDOW + 32, :]],
                    axis=1,
                ).astype(f32)
            else:
                tail = gated_rows(at - 16, 16)
            before2, before1 = tail[14:15, :], tail[15:16, :]
            g = gated_rows(at, WINDOW)
            one = jnp.where(row == 0, before1, pltpu.roll(g, 1, 0))
            two = jnp.where(row == 0, before2, jnp.where(row == 1, before1, pltpu.roll(g, 2, 0)))
            convolved = two * t[0:1] + one * t[1:2] + g * t[2:3]
            out_gate = proj[side, 0, at : at + WINDOW, 0:chans].astype(f32)
            acts[to : to + WINDOW, base : base + chans] = (out_gate * convolved).astype(bf16)

            kv_cols = slice(side * pair, (side + 1) * pair)
            kv_here = kv_rows[0, at : at + WINDOW, kv_cols]
            if n == 0:
                kv_before = edge[side, 0, 0:WINDOW, :]
            else:
                kv_before = kv_rows[0, at - WINDOW : at, kv_cols]
            kv = jnp.concatenate([kv_before, kv_here], axis=0)
            keys = lax.dot_general(pick_kt, kv, transposed, preferred_element_type=f32).astype(bf16)
            values = jnp.dot(kv, pick_v, preferred_element_type=f32).astype(bf16)
            values = jnp.concatenate([values, ones], axis=1)
            q = proj[side, 0, at : at + WINDOW, q_at : q_at + chans]
            allowed = first if n == 0 else band
            outs = []
            for h in range(heads):
                qh = jnp.where((lane >= h * HEAD) & (lane < (h + 1) * HEAD), q, jnp.zeros_like(q))
                sc = jnp.dot(qh, keys, preferred_element_type=f32)
                sc = jnp.where(allowed, sc * (1.0 / 8.0), -jnp.inf)
                sink = sinks[side, h]
                m = jnp.maximum(jnp.max(sc, axis=1, keepdims=True), sink)
                e = jnp.exp(sc - m).astype(bf16)
                o = jnp.dot(e, values, preferred_element_type=f32)
                outs.append(o[:, :pair] / (o[:, pair:] + jnp.exp(sink - m)))
            for j in range(heads // 2):
                col = base + chans + j * pair
                acts[to : to + WINDOW, col : col + pair] = jnp.where(
                    left, outs[2 * j], outs[2 * j + 1]
                ).astype(bf16)

    wanted.wait()
    product = jnp.dot(acts[...], wo[...], preferred_element_type=f32)
    if arrived:
        product = product + jnp.concatenate([a[...] for a in arrived], axis=0).astype(f32)
    product = product.astype(bf16)
    at = 0
    for ref in results:
        ref[...] = product[at : at + ref.shape[0]]
        at += ref.shape[0]


def added(*parts):
    total = parts[0].astype(jnp.float32)
    for p in parts[1:]:
        total = total + p.astype(jnp.float32)
    return total.astype(jnp.bfloat16)


def layer(
    tokens,
    norm_gain,
    w_bgate,
    w_cgate,
    w_conv_in,
    conv_taps,
    w_query,
    w_key,
    w_value,
    sink_logits,
    conv_out_weight,
    attn_out_weight,
):
    fs = lax.axis_size("fs")
    sp = lax.axis_size("sp")
    tp = lax.axis_size("tp")
    bf16, f32 = jnp.bfloat16, jnp.float32
    rows_in = w_bgate.shape[0]
    chans = w_bgate.shape[1] // fs
    block = rows_in * fs
    b_width, out_cols = 3 * chans, 2 * chans
    in_cols = b_width + chans + 2 * HEAD
    width = in_cols + out_cols
    packed = pl.pallas_call(
        pack_kernel,
        out_shape=jax.ShapeDtypeStruct((fs, rows_in, width), bf16),
        in_specs=[VMEM] * 8,
        out_specs=VMEM,
        name="pack_weights",
    )(w_query, w_key, w_value, conv_out_weight.T, attn_out_weight.T, w_bgate, w_cgate, w_conv_in)
    mine = lax.all_to_all(packed, "fs", split_axis=0, concat_axis=0, tiled=True)
    mine = pl.pallas_call(
        functools.partial(turn_kernel, in_cols),
        out_shape=jax.ShapeDtypeStruct((block, width), bf16),
        in_specs=[VMEM],
        out_specs=VMEM,
        name="turn_weights",
    )(mine.reshape(block, width))
    weights = lax.all_gather(mine, ("sp", "tp"), axis=0, tiled=True)
    weights = weights.reshape(sp, tp, block, width)

    core, place, group = lax.axis_index("tp"), lax.axis_index("sp"), lax.axis_index("fs")
    heads = chans // HEAD
    idx = jnp.stack([place * tp + core, place]).astype(jnp.int32)
    taps = lax.dynamic_slice_in_dim(conv_taps, group * chans, chans, 1).astype(f32)
    sinks = lax.dynamic_slice_in_dim(sink_logits, group * heads, heads, 0)
    small = jnp.concatenate([taps, jnp.pad(sinks[None], ((0, 0), (0, chans - heads)))], axis=0)

    widened = tokens[0].astype(f32)
    normed = (
        widened
        * lax.rsqrt(jnp.mean(widened * widened, axis=-1, keepdims=True) + EPSILON)
        * norm_gain
    ).astype(bf16)
    here, feats = normed.shape
    half = here // 2
    prev = ring(normed, "fs", 1)
    succ = ring(normed, "fs", -1)
    opp_a = ring(prev[:half], "fs", 1)
    opp_b = ring(succ[half:], "fs", -1)
    theirs = lax.ppermute(small, "tp", [(0, 1), (1, 0)])
    both = jnp.where(core == 0, jnp.stack([small, theirs]), jnp.stack([theirs, small]))
    taps, sinks = both[:, :TAPS], both[:, TAPS, :heads]
    weights, idx, taps, sinks = lax.optimization_barrier((weights, idx, taps, sinks))

    squares = out_cols // block
    pair = 2 * HEAD
    proj, kvs, edge, wout = pl.pallas_call(
        functools.partial(project_kernel, b_width),
        out_shape=(
            jax.ShapeDtypeStruct((tp, fs, here, in_cols - pair), bf16),
            jax.ShapeDtypeStruct((fs, here, tp * pair), bf16),
            jax.ShapeDtypeStruct((tp, fs, WINDOW + 32, 2 * HEAD), bf16),
            jax.ShapeDtypeStruct((tp * out_cols, feats), bf16),
        ),
        grid=(tp,),
        in_specs=[ANY] * 6,
        out_specs=(
            pl.BlockSpec((1, fs, here, in_cols - pair), lambda t: (t, 0, 0, 0)),
            pl.BlockSpec((fs, here, tp * pair), lambda t: (0, 0, 0)),
            pl.BlockSpec((tp, fs, WINDOW + 32, pair), lambda t: (0, 0, 0, 0)),
            ANY,
        ),
        scratch_shapes=[
            pltpu.VMEM((fs, here, feats), bf16),
            pltpu.VMEM((tp, sp, block, in_cols - pair), bf16),
            pltpu.VMEM((sp, block, tp * pair), bf16),
            pltpu.VMEM((tp * out_cols, feats), bf16),
            pltpu.SemaphoreType.DMA((10 + tp * squares * sp,)),
        ],
        cost_estimate=pl.CostEstimate(
            flops=2 * tp * fs * here * feats * in_cols, bytes_accessed=25_000_000, transcendentals=0
        ),
        compiler_params=pltpu.CompilerParams(dimension_semantics=("arbitrary",)),
        name="project_rows",
    )(weights, opp_a, opp_b, succ, prev, normed)
    edge = lax.ppermute(edge, ("sp", "tp"), [(i, i + 1) for i in range(sp * tp - 1)])

    def mix(tasks, pieces, arrived=()):
        seqs, blocks = zip(*tasks)
        edged = [q for q, n in tasks if n == 0]

        def part(shape, q):
            return pl.BlockSpec((tp, 1) + shape, lambda i, q=q: (0, q, 0, 0))

        return pl.pallas_call(
            functools.partial(mix_kernel, blocks, pieces, b_width),
            out_shape=tuple(jax.ShapeDtypeStruct((n, feats), bf16) for n in pieces),
            grid=(1,),
            in_specs=[SMEM, SMEM, pl.BlockSpec((tp, TAPS, chans), lambda i: (0, 0, 0)), ANY]
            + [part((here, in_cols - pair), q) for q in seqs]
            + [pl.BlockSpec((1, here, tp * pair), lambda i, q=q: (q, 0, 0)) for q in seqs]
            + [part((WINDOW + 32, 2 * HEAD), q) for q in (seqs if edged else ())]
            + [pl.BlockSpec(a.shape, lambda i: (0, 0)) for a in arrived],
            out_specs=tuple(pl.BlockSpec((n, feats), lambda i: (0, 0)) for n in pieces),
            scratch_shapes=[
                pltpu.VMEM((here, tp * out_cols), bf16),
                pltpu.VMEM((tp * out_cols, feats), bf16),
                pltpu.SemaphoreType.DMA,
            ],
            cost_estimate=pl.CostEstimate(
                flops=2 * here * feats * tp * out_cols + 600_000_000,
                bytes_accessed=8_000_000,
                transcendentals=600_000,
            ),
        )(idx, sinks, taps, wout, proj, proj, kvs, kvs, *((edge, edge) if edged else ()), *arrived)

    def sent(array, by):
        return ring(array, "fs", by)

    succ_q, prev_q, opp_q, own_q = range(4)
    low, high = mix(((succ_q, 1), (opp_q, 1)), (half, half))
    down, up_b = sent(high, -1), sent(low, 1)
    quarter = half // 2
    low_1, low_2, high = mix(((opp_q, 0), (prev_q, 0)), (quarter, quarter, half))
    up_1, up_2 = sent(low_1, 1), sent(low_2, 1)
    down_a = sent(high, -1)
    low_1, low_2, high = mix(((succ_q, 0), (prev_q, 1)), (quarter, quarter, half))
    down_b = sent(added(high, down), -1)
    up_a1, up_a2 = sent(added(low_1, up_1), 1), sent(added(low_2, up_2), 1)
    (own,) = mix(((own_q, 0), (own_q, 1)), (here,), (down_a, up_b))
    return added(own, jnp.concatenate([up_a1, up_a2, down_b], 0))[None]


def solution(mesh):
    placed = (
        P(("grp", "fs"), ("sp", "tp"), None),
        P(),
        P(("sp", "fs"), "tp"),
        P(("sp", "fs"), "tp"),
        P(("sp", "fs"), "tp"),
        P(None, "tp"),
        P(("sp", "fs"), "tp"),
        P(("sp", "fs"), "tp"),
        P(("sp", "fs"), "tp"),
        P("tp"),
        P("tp", ("sp", "fs")),
        P("tp", ("sp", "fs")),
    )
    return jax.shard_map(
        layer,
        mesh=mesh,
        in_specs=placed,
        out_specs=P(("grp", "fs"), ("sp", "tp"), None),
        check_vma=False,
    )
```

```python
import functools

import jax
import jax.numpy as jnp
from jax import lax
from jax.experimental import pallas as pl
from jax.experimental.pallas import tpu as pltpu
from jax.sharding import PartitionSpec as P


HEAD = 64
WINDOW = 128
TAPS = 3
EPSILON = 1e-06
LOG2_E = 1.4426950408889634


ANY = pl.BlockSpec(memory_space=pl.ANY)
SMEM = pl.BlockSpec(memory_space=pltpu.SMEM)
VMEM = pl.BlockSpec(memory_space=pltpu.VMEM)


def ring(array, axis, by):
    size = lax.axis_size(axis)
    return lax.ppermute(array, axis, [(i, (i + by) % size) for i in range(size)])


def pack_kernel(group, wq, wk, wv, conv_t, attn_t, wb, wc, wi, *outs):
    fs = len(outs)
    chans = wq.shape[1] // fs
    for d, out in enumerate(outs):
        to = lax.rem(group[0] + d, fs)
        cut = pl.ds(pl.multiple_of(to * chans, chans), chans)
        second = to >= fs // 2
        kv = jnp.concatenate(
            [jnp.where(second, w[:, HEAD : 2 * HEAD], w[:, :HEAD]) for w in (wk, wv)], axis=1
        )
        at = 0
        for part in (wb[:, cut], wc[:, cut], wi[:, cut], wq[:, cut], kv, conv_t[:, cut], attn_t[:, cut]):
            out[:, at : at + part.shape[1]] = part
            at += part.shape[1]


def turn_kernel(in_cols, group, *refs):
    parts, out, squares = refs[:-2], refs[-2], refs[-1]
    block, width = out.shape
    rows = parts[0].shape[0]
    for d, part in enumerate(parts):
        source = lax.rem(group[0] - d + len(parts), len(parts))
        at = pl.ds(pl.multiple_of(source * rows, rows), rows)
        out[at, :in_cols] = part[:, :in_cols]
        squares[at, :] = part[:, in_cols:]
    for at in range(0, width - in_cols, block):
        out[:, in_cols + at : in_cols + at + block] = squares[:, at : at + block].T


def project_kernel(wide, weights, *refs):
    opp_a, opp_b, succ, prev, own, out, kvs, edge, wout, xs, ws, wkv, wo, sems = refs
    step = pl.program_id(0)
    half = opp_a.shape[0]
    block = weights.shape[2]
    blocks = weights.shape[0]
    main = ws.shape[3]
    pair = wkv.shape[2] // 2
    parts = (weights.shape[3] - main - pair) // block
    bf16, f32 = jnp.bfloat16, jnp.float32
    x_copies = [
        pltpu.make_async_copy(ref, xs.at[s, pl.ds(at, ref.shape[0]), :], sems.at[i])
        for i, (ref, s, at) in enumerate(
            ((succ, 0, 0), (prev, 1, 0), (opp_a, 2, 0), (opp_b, 2, half), (own, 3, 0))
        )
    ]
    w_copies = [
        pltpu.make_async_copy(weights.at[:, t, :, pl.ds(0, main)], ws.at[t], sems.at[5 + t])
        for t in range(2)
    ]
    kv_copies = [
        pltpu.make_async_copy(
            weights.at[:, t, :, pl.ds(main, pair)], wkv.at[:, :, pl.ds(t * pair, pair)], sems.at[7 + t]
        )
        for t in range(2)
    ]
    out_copies = [
        pltpu.make_async_copy(
            weights.at[j, t, :, pl.ds(main + pair + b * block, block)],
            wo.at[pl.ds((t * parts + b) * block, block), pl.ds(j * block, block)],
            sems.at[9 + (t * parts + b) * blocks + j],
        )
        for t in range(2)
        for b in range(parts)
        for j in range(blocks)
    ]
    laid_out = pltpu.make_async_copy(wo, wout, sems.at[9 + 2 * parts * blocks])

    @pl.when(step == 0)
    def _():
        for c in x_copies + w_copies[:1]:
            c.start()
        for c in x_copies + w_copies[:1]:
            c.wait()
        for c in w_copies[1:] + kv_copies + out_copies:
            c.start()

    @pl.when(step == 1)
    def _():
        for c in w_copies[1:] + kv_copies + out_copies:
            c.wait()
        laid_out.start()

    seqs, length, feats = xs.shape
    x = xs[...].reshape(seqs * length, feats)
    w = ws[step].reshape(feats, main)
    rounded = jnp.dot(x, w, preferred_element_type=f32).astype(bf16).reshape(seqs, length, main)
    out[0] = rounded
    chans = wide // 3
    for s in range(seqs):
        last = rounded[s, length - 16 :, chans:wide].astype(f32)
        gated = (last[:, :chans] * last[:, chans:]).astype(bf16)
        edge[step, s, WINDOW : WINDOW + 16, :] = gated[:, : 2 * HEAD]
        edge[step, s, WINDOW + 16 : WINDOW + 32, :] = gated[:, 2 * HEAD :]

    @pl.when(step == 1)
    def _():
        k = wkv[...].reshape(feats, 2 * pair)
        both = jnp.dot(x, k, preferred_element_type=f32).astype(bf16).reshape(seqs, length, 2 * pair)
        kvs[...] = both
        for t in range(2):
            for s in range(seqs):
                edge[t, s, 0:WINDOW, :] = both[s, length - WINDOW :, t * pair : (t + 1) * pair]
        laid_out.wait()


def mix_kernel(blocks, pieces, wide, idx, sinks, taps, wout, *refs):
    acts, wo, sem = refs[-3:]
    outs_at = len(refs) - 3 - len(pieces)
    results = refs[outs_at:-3]
    has_edge = 2 if 0 in blocks else 0
    projs, kvs, edges = refs[:2], refs[2:4], refs[4 : 4 + has_edge]
    arrived = refs[4 + has_edge : outs_at]
    wanted = pltpu.make_async_copy(wout, wo, sem)
    wanted.start()
    place = idx[0]
    chans = wide // 3
    heads = chans // HEAD
    f32, bf16 = jnp.float32, jnp.bfloat16
    q_at = wide
    pair = 2 * HEAD

    def iota(shape, dim):
        return lax.broadcasted_iota(jnp.int32, shape, dim)

    pick_kt = (iota((chans, pair), 1) == jnp.bitwise_and(iota((chans, pair), 0), HEAD - 1)).astype(bf16)
    pick_v = (iota((pair, pair), 0) == jnp.bitwise_and(iota((pair, pair), 1), HEAD - 1) + HEAD).astype(bf16)
    row = iota((WINDOW, chans), 0)
    lane = iota((WINDOW, chans), 1)
    left = iota((WINDOW, pair), 1) < HEAD
    qi, ki = iota((WINDOW, 2 * WINDOW), 0), iota((WINDOW, 2 * WINDOW), 1)
    band = (ki > qi) & (ki <= qi + WINDOW)
    first = band & ((ki >= WINDOW) | (place > 0))
    ones = jnp.ones((2 * WINDOW, pair), bf16)
    transposed = (((1,), (1,)), ((), ()))
    for slot, n in enumerate(blocks):
        at, to = n * WINDOW, slot * WINDOW
        proj, kv_rows, edge = projs[slot], kvs[slot], edges[slot] if n == 0 else None
        for side in range(2):

            def gated_rows(start, rows):
                c = proj[side, 0, start : start + rows, chans : 2 * chans].astype(f32)
                i = proj[side, 0, start : start + rows, 2 * chans : 3 * chans].astype(f32)
                return (c * i).astype(bf16).astype(f32)

            t = taps[side]
            base = side * 2 * chans
            if n == 0:
                tail = jnp.concatenate(
                    [edge[side, 0, WINDOW : WINDOW + 16, :], edge[side, 0, WINDOW + 16 : WINDOW + 32, :]],
                    axis=1,
                ).astype(f32)
            else:
                tail = gated_rows(at - 16, 16)
            before2, before1 = tail[14:15, :], tail[15:16, :]
            g = gated_rows(at, WINDOW)
            one = jnp.where(row == 0, before1, pltpu.roll(g, 1, 0))
            two = jnp.where(row == 0, before2, jnp.where(row == 1, before1, pltpu.roll(g, 2, 0)))
            convolved = two * t[0:1] + one * t[1:2] + g * t[2:3]
            out_gate = proj[side, 0, at : at + WINDOW, 0:chans].astype(f32)
            acts[to : to + WINDOW, base : base + chans] = (out_gate * convolved).astype(bf16)

            kv_cols = slice(side * pair, (side + 1) * pair)
            kv_here = kv_rows[0, at : at + WINDOW, kv_cols]
            if n == 0:
                kv_before = edge[side, 0, 0:WINDOW, :]
            else:
                kv_before = kv_rows[0, at - WINDOW : at, kv_cols]
            kv = jnp.concatenate([kv_before, kv_here], axis=0)
            keys = lax.dot_general(pick_kt, kv, transposed, preferred_element_type=f32).astype(bf16)
            values = jnp.dot(kv, pick_v, preferred_element_type=f32).astype(bf16)
            values = jnp.concatenate([values, ones], axis=1)
            q = proj[side, 0, at : at + WINDOW, q_at : q_at + chans]
            allowed = first if n == 0 else band
            outs = []
            for h in range(heads):
                qh = jnp.where((lane >= h * HEAD) & (lane < (h + 1) * HEAD), q, jnp.zeros_like(q))
                sc = jnp.dot(qh, keys, preferred_element_type=f32)
                sc = jnp.where(allowed, sc * (LOG2_E / 8.0), -jnp.inf)
                sink = sinks[side, h] * LOG2_E
                m = jnp.maximum(jnp.max(sc, axis=1, keepdims=True), sink)
                e = jnp.exp2(sc - m).astype(bf16)
                o = jnp.dot(e, values, preferred_element_type=f32)
                outs.append(o[:, :pair] / (o[:, pair:] + jnp.exp2(sink - m)))
            for j in range(heads // 2):
                col = base + chans + j * pair
                acts[to : to + WINDOW, col : col + pair] = jnp.where(
                    left, outs[2 * j], outs[2 * j + 1]
                ).astype(bf16)

    wanted.wait()
    product = jnp.dot(acts[...], wo[...], preferred_element_type=f32)
    if arrived:
        product = product + jnp.concatenate([a[...] for a in arrived], axis=0).astype(f32)
    product = product.astype(bf16)
    at = 0
    for ref in results:
        ref[...] = product[at : at + ref.shape[0]]
        at += ref.shape[0]


def added(*parts):
    total = parts[0].astype(jnp.float32)
    for p in parts[1:]:
        total = total + p.astype(jnp.float32)
    return total.astype(jnp.bfloat16)


def layer(
    tokens,
    norm_gain,
    w_bgate,
    w_cgate,
    w_conv_in,
    conv_taps,
    w_query,
    w_key,
    w_value,
    sink_logits,
    conv_out_weight,
    attn_out_weight,
):
    fs = lax.axis_size("fs")
    sp = lax.axis_size("sp")
    tp = lax.axis_size("tp")
    bf16, f32 = jnp.bfloat16, jnp.float32
    rows_in = w_bgate.shape[0]
    chans = w_bgate.shape[1] // fs
    block = rows_in * fs
    b_width, out_cols = 3 * chans, 2 * chans
    in_cols = b_width + chans + 2 * HEAD
    width = in_cols + out_cols
    core, place, group = lax.axis_index("tp"), lax.axis_index("sp"), lax.axis_index("fs")
    idx = (place * tp + core).astype(jnp.int32).reshape(1)
    member = group.astype(jnp.int32).reshape(1)
    packed = pl.pallas_call(
        pack_kernel,
        out_shape=(jax.ShapeDtypeStruct((rows_in, width), bf16),) * fs,
        in_specs=[SMEM] + [VMEM] * 8,
        out_specs=(VMEM,) * fs,
        name="pack_weights",
    )(member, w_query, w_key, w_value, conv_out_weight.T, attn_out_weight.T, w_bgate, w_cgate, w_conv_in)
    mine = pl.pallas_call(
        functools.partial(turn_kernel, in_cols),
        out_shape=jax.ShapeDtypeStruct((block, width), bf16),
        in_specs=[SMEM] + [VMEM] * fs,
        out_specs=VMEM,
        scratch_shapes=[pltpu.VMEM((block, out_cols), bf16)],
        name="turn_weights",
    )(member, packed[0], *(ring(p, "fs", d) for d, p in enumerate(packed) if d > 0))
    weights = lax.all_gather(mine, ("sp", "tp"), axis=0, tiled=True)
    weights = weights.reshape(sp, tp, block, width)

    heads = chans // HEAD
    taps = lax.dynamic_slice_in_dim(conv_taps, group * chans, chans, 1).astype(f32)
    sinks = lax.dynamic_slice_in_dim(sink_logits, group * heads, heads, 0)
    small = jnp.concatenate([taps, jnp.pad(sinks[None], ((0, 0), (0, chans - heads)))], axis=0)

    widened = tokens[0].astype(f32)
    normed = (
        widened
        * lax.rsqrt(jnp.mean(widened * widened, axis=-1, keepdims=True) + EPSILON)
        * norm_gain
    ).astype(bf16)
    here, feats = normed.shape
    half = here // 2
    prev = ring(normed, "fs", 1)
    succ = ring(normed, "fs", -1)
    opp_a = ring(prev[:half], "fs", 1)
    opp_b = ring(succ[half:], "fs", -1)
    theirs = lax.ppermute(small, "tp", [(0, 1), (1, 0)])
    both = jnp.where(core == 0, jnp.stack([small, theirs]), jnp.stack([theirs, small]))
    taps, sinks = both[:, :TAPS], both[:, TAPS, :heads]
    weights, idx, taps, sinks = lax.optimization_barrier((weights, idx, taps, sinks))

    squares = out_cols // block
    pair = 2 * HEAD
    proj, kvs, edge, wout = pl.pallas_call(
        functools.partial(project_kernel, b_width),
        out_shape=(
            jax.ShapeDtypeStruct((tp, fs, here, in_cols - pair), bf16),
            jax.ShapeDtypeStruct((fs, here, tp * pair), bf16),
            jax.ShapeDtypeStruct((tp, fs, WINDOW + 32, 2 * HEAD), bf16),
            jax.ShapeDtypeStruct((tp * out_cols, feats), bf16),
        ),
        grid=(tp,),
        in_specs=[ANY] * 6,
        out_specs=(
            pl.BlockSpec((1, fs, here, in_cols - pair), lambda t: (t, 0, 0, 0)),
            pl.BlockSpec((fs, here, tp * pair), lambda t: (0, 0, 0)),
            pl.BlockSpec((tp, fs, WINDOW + 32, pair), lambda t: (0, 0, 0, 0)),
            ANY,
        ),
        scratch_shapes=[
            pltpu.VMEM((fs, here, feats), bf16),
            pltpu.VMEM((tp, sp, block, in_cols - pair), bf16),
            pltpu.VMEM((sp, block, tp * pair), bf16),
            pltpu.VMEM((tp * out_cols, feats), bf16),
            pltpu.SemaphoreType.DMA((10 + tp * squares * sp,)),
        ],
        cost_estimate=pl.CostEstimate(
            flops=2 * tp * fs * here * feats * in_cols, bytes_accessed=25_000_000, transcendentals=0
        ),
        compiler_params=pltpu.CompilerParams(dimension_semantics=("arbitrary",)),
        name="project_rows",
    )(weights, opp_a, opp_b, succ, prev, normed)
    edge = lax.ppermute(edge, ("sp", "tp"), [(i, i + 1) for i in range(sp * tp - 1)])

    def mix(tasks, pieces, arrived=()):
        seqs, blocks = zip(*tasks)
        edged = [q for q, n in tasks if n == 0]

        def part(shape, q):
            return pl.BlockSpec((tp, 1) + shape, lambda i, q=q: (0, q, 0, 0))

        return pl.pallas_call(
            functools.partial(mix_kernel, blocks, pieces, b_width),
            out_shape=tuple(jax.ShapeDtypeStruct((n, feats), bf16) for n in pieces),
            grid=(1,),
            in_specs=[SMEM, SMEM, pl.BlockSpec((tp, TAPS, chans), lambda i: (0, 0, 0)), ANY]
            + [part((here, in_cols - pair), q) for q in seqs]
            + [pl.BlockSpec((1, here, tp * pair), lambda i, q=q: (q, 0, 0)) for q in seqs]
            + [part((WINDOW + 32, 2 * HEAD), q) for q in (seqs if edged else ())]
            + [pl.BlockSpec(a.shape, lambda i: (0, 0)) for a in arrived],
            out_specs=tuple(pl.BlockSpec((n, feats), lambda i: (0, 0)) for n in pieces),
            scratch_shapes=[
                pltpu.VMEM((here, tp * out_cols), bf16),
                pltpu.VMEM((tp * out_cols, feats), bf16),
                pltpu.SemaphoreType.DMA,
            ],
            cost_estimate=pl.CostEstimate(
                flops=2 * here * feats * tp * out_cols + 600_000_000,
                bytes_accessed=8_000_000,
                transcendentals=600_000,
            ),
        )(idx, sinks, taps, wout, proj, proj, kvs, kvs, *((edge, edge) if edged else ()), *arrived)

    def sent(array, by):
        return ring(array, "fs", by)

    succ_q, prev_q, opp_q, own_q = range(4)
    low, high = mix(((succ_q, 1), (opp_q, 1)), (half, half))
    down, up_b = sent(high, -1), sent(low, 1)
    quarter = half // 2
    low_1, low_2, high = mix(((opp_q, 0), (prev_q, 0)), (quarter, quarter, half))
    up_1, up_2 = sent(low_1, 1), sent(low_2, 1)
    down_a = sent(high, -1)
    low_1, low_2, high = mix(((succ_q, 0), (prev_q, 1)), (quarter, quarter, half))
    down_b = sent(added(high, down), -1)
    up_a1, up_a2 = sent(added(low_1, up_1), 1), sent(added(low_2, up_2), 1)
    (own,) = mix(((own_q, 0), (own_q, 1)), (here,), (down_a, up_b))
    return added(own, jnp.concatenate([up_a1, up_a2, down_b], 0))[None]


def solution(mesh):
    placed = (
        P(("grp", "fs"), ("sp", "tp"), None),
        P(),
        P(("sp", "fs"), "tp"),
        P(("sp", "fs"), "tp"),
        P(("sp", "fs"), "tp"),
        P(None, "tp"),
        P(("sp", "fs"), "tp"),
        P(("sp", "fs"), "tp"),
        P(("sp", "fs"), "tp"),
        P("tp"),
        P("tp", ("sp", "fs")),
        P("tp", ("sp", "fs")),
    )
    return jax.shard_map(
        layer,
        mesh=mesh,
        in_specs=placed,
        out_specs=P(("grp", "fs"), ("sp", "tp"), None),
        check_vma=False,
    )
```

```python
import functools

import jax
import jax.numpy as jnp
from jax import lax
from jax.experimental import pallas as pl
from jax.experimental.pallas import tpu as pltpu
from jax.sharding import PartitionSpec as P


HEAD = 64
WINDOW = 128
TAPS = 3
EPSILON = 1e-06


ANY = pl.BlockSpec(memory_space=pl.ANY)
SMEM = pl.BlockSpec(memory_space=pltpu.SMEM)
VMEM = pl.BlockSpec(memory_space=pltpu.VMEM)


def ring(array, axis, by):
    size = lax.axis_size(axis)
    return lax.ppermute(array, axis, [(i, (i + by) % size) for i in range(size)])


def pack_kernel(group, wq, wk, wv, conv_t, attn_t, wb, wc, wi, *outs):
    fs = len(outs)
    chans = wq.shape[1] // fs
    for d, out in enumerate(outs):
        to = lax.rem(group[0] + d, fs)
        cut = pl.ds(pl.multiple_of(to * chans, chans), chans)
        second = to >= fs // 2
        kv = jnp.concatenate(
            [jnp.where(second, w[:, HEAD : 2 * HEAD], w[:, :HEAD]) for w in (wk, wv)], axis=1
        )
        at = 0
        for part in (wb[:, cut], wc[:, cut], wi[:, cut], wq[:, cut], kv, conv_t[:, cut], attn_t[:, cut]):
            out[:, at : at + part.shape[1]] = part
            at += part.shape[1]


def turn_kernel(in_cols, group, *refs):
    parts, out, squares = refs[:-2], refs[-2], refs[-1]
    block, width = out.shape
    rows = parts[0].shape[0]
    for d, part in enumerate(parts):
        source = lax.rem(group[0] - d + len(parts), len(parts))
        at = pl.ds(pl.multiple_of(source * rows, rows), rows)
        out[at, :in_cols] = part[:, :in_cols]
        squares[at, :] = part[:, in_cols:]
    for at in range(0, width - in_cols, block):
        out[:, in_cols + at : in_cols + at + block] = squares[:, at : at + block].T


def project_kernel(wide, weights, *refs):
    opp_a, opp_b, succ, prev, own, out, kvs, edge, wout, xs, ws, wkv, wo, sems = refs
    step = pl.program_id(0)
    half = opp_a.shape[0]
    block = weights.shape[2]
    blocks = weights.shape[0]
    main = ws.shape[3]
    pair = wkv.shape[2] // 2
    parts = (weights.shape[3] - main - pair) // block
    bf16, f32 = jnp.bfloat16, jnp.float32
    x_copies = [
        pltpu.make_async_copy(ref, xs.at[s, pl.ds(at, ref.shape[0]), :], sems.at[i])
        for i, (ref, s, at) in enumerate(
            ((succ, 0, 0), (prev, 1, 0), (opp_a, 2, 0), (opp_b, 2, half), (own, 3, 0))
        )
    ]
    w_copies = [
        pltpu.make_async_copy(weights.at[:, t, :, pl.ds(0, main)], ws.at[t], sems.at[5 + t])
        for t in range(2)
    ]
    kv_copies = [
        pltpu.make_async_copy(
            weights.at[:, t, :, pl.ds(main, pair)], wkv.at[:, :, pl.ds(t * pair, pair)], sems.at[7 + t]
        )
        for t in range(2)
    ]
    out_copies = [
        pltpu.make_async_copy(
            weights.at[j, t, :, pl.ds(main + pair + b * block, block)],
            wo.at[pl.ds((t * parts + b) * block, block), pl.ds(j * block, block)],
            sems.at[9 + (t * parts + b) * blocks + j],
        )
        for t in range(2)
        for b in range(parts)
        for j in range(blocks)
    ]
    laid_out = pltpu.make_async_copy(wo, wout, sems.at[9 + 2 * parts * blocks])

    @pl.when(step == 0)
    def _():
        for c in x_copies + w_copies[:1]:
            c.start()
        for c in x_copies + w_copies[:1]:
            c.wait()
        for c in w_copies[1:] + kv_copies + out_copies:
            c.start()

    @pl.when(step == 1)
    def _():
        for c in w_copies[1:] + kv_copies + out_copies:
            c.wait()
        laid_out.start()

    seqs, length, feats = xs.shape
    x = xs[...].reshape(seqs * length, feats)
    w = ws[step].reshape(feats, main)
    rounded = jnp.dot(x, w, preferred_element_type=f32).astype(bf16).reshape(seqs, length, main)
    out[0] = rounded
    chans = wide // 3
    for s in range(seqs):
        last = rounded[s, length - 16 :, chans:wide].astype(f32)
        gated = (last[:, :chans] * last[:, chans:]).astype(bf16)
        edge[step, s, WINDOW : WINDOW + 16, :] = gated[:, : 2 * HEAD]
        edge[step, s, WINDOW + 16 : WINDOW + 32, :] = gated[:, 2 * HEAD :]

    @pl.when(step == 1)
    def _():
        k = wkv[...].reshape(feats, 2 * pair)
        both = jnp.dot(x, k, preferred_element_type=f32).astype(bf16).reshape(seqs, length, 2 * pair)
        kvs[...] = both
        for t in range(2):
            for s in range(seqs):
                edge[t, s, 0:WINDOW, :] = both[s, length - WINDOW :, t * pair : (t + 1) * pair]
        laid_out.wait()


def mix_kernel(blocks, pieces, wide, idx, sinks, taps, wout, *refs):
    acts, wo, sem = refs[-3:]
    outs_at = len(refs) - 3 - len(pieces)
    results = refs[outs_at:-3]
    has_edge = 2 if 0 in blocks else 0
    projs, kvs, edges = refs[:2], refs[2:4], refs[4 : 4 + has_edge]
    arrived = refs[4 + has_edge : outs_at]
    wanted = pltpu.make_async_copy(wout, wo, sem)
    wanted.start()
    place = idx[0]
    chans = wide // 3
    heads = chans // HEAD
    f32, bf16 = jnp.float32, jnp.bfloat16
    q_at = wide
    pair = 2 * HEAD

    def iota(shape, dim):
        return lax.broadcasted_iota(jnp.int32, shape, dim)

    pick_kt = (iota((chans, pair), 1) == jnp.bitwise_and(iota((chans, pair), 0), HEAD - 1)).astype(bf16)
    pick_v = (iota((pair, pair), 0) == jnp.bitwise_and(iota((pair, pair), 1), HEAD - 1) + HEAD).astype(bf16)
    row = iota((WINDOW, chans), 0)
    lane = iota((WINDOW, chans), 1)
    left = iota((WINDOW, pair), 1) < HEAD
    qi, ki = iota((WINDOW, 2 * WINDOW), 0), iota((WINDOW, 2 * WINDOW), 1)
    band = (ki > qi) & (ki <= qi + WINDOW)
    first = band & ((ki >= WINDOW) | (place > 0))
    ones = jnp.ones((2 * WINDOW, pair), bf16)
    transposed = (((1,), (1,)), ((), ()))
    for slot, n in enumerate(blocks):
        at, to = n * WINDOW, slot * WINDOW
        proj, kv_rows, edge = projs[slot], kvs[slot], edges[slot] if n == 0 else None
        for side in range(2):

            def gated_rows(start, rows):
                c = proj[side, 0, start : start + rows, chans : 2 * chans].astype(f32)
                i = proj[side, 0, start : start + rows, 2 * chans : 3 * chans].astype(f32)
                return (c * i).astype(bf16).astype(f32)

            t = taps[side]
            base = side * 2 * chans
            if n == 0:
                tail = jnp.concatenate(
                    [edge[side, 0, WINDOW : WINDOW + 16, :], edge[side, 0, WINDOW + 16 : WINDOW + 32, :]],
                    axis=1,
                ).astype(f32)
            else:
                tail = gated_rows(at - 16, 16)
            before2, before1 = tail[14:15, :], tail[15:16, :]
            g = gated_rows(at, WINDOW)
            one = jnp.where(row == 0, before1, pltpu.roll(g, 1, 0))
            two = jnp.where(row == 0, before2, jnp.where(row == 1, before1, pltpu.roll(g, 2, 0)))
            convolved = two * t[0:1] + one * t[1:2] + g * t[2:3]
            out_gate = proj[side, 0, at : at + WINDOW, 0:chans].astype(f32)
            acts[to : to + WINDOW, base : base + chans] = (out_gate * convolved).astype(bf16)

            kv_cols = slice(side * pair, (side + 1) * pair)
            kv_here = kv_rows[0, at : at + WINDOW, kv_cols]
            if n == 0:
                kv_before = edge[side, 0, 0:WINDOW, :]
            else:
                kv_before = kv_rows[0, at - WINDOW : at, kv_cols]
            kv = jnp.concatenate([kv_before, kv_here], axis=0)
            keys = lax.dot_general(pick_kt, kv, transposed, preferred_element_type=f32).astype(bf16)
            values = jnp.dot(kv, pick_v, preferred_element_type=f32).astype(bf16)
            values = jnp.concatenate([values, ones], axis=1)
            q = proj[side, 0, at : at + WINDOW, q_at : q_at + chans]
            allowed = first if n == 0 else band
            outs = []
            for h in range(heads):
                qh = jnp.where((lane >= h * HEAD) & (lane < (h + 1) * HEAD), q, jnp.zeros_like(q))
                sc = jnp.dot(qh, keys, preferred_element_type=f32)
                sc = jnp.where(allowed, sc * (1.0 / 8.0), -jnp.inf)
                sink = sinks[side, h]
                m = jnp.maximum(jnp.max(sc, axis=1, keepdims=True), sink)
                e = jnp.exp(sc - m).astype(bf16)
                o = jnp.dot(e, values, preferred_element_type=f32)
                outs.append(o[:, :pair] / (o[:, pair:] + jnp.exp(sink - m)))
            for j in range(heads // 2):
                col = base + chans + j * pair
                acts[to : to + WINDOW, col : col + pair] = jnp.where(
                    left, outs[2 * j], outs[2 * j + 1]
                ).astype(bf16)

    wanted.wait()
    product = jnp.dot(acts[...], wo[...], preferred_element_type=f32)
    if arrived:
        product = product + jnp.concatenate([a[...] for a in arrived], axis=0).astype(f32)
    product = product.astype(bf16)
    at = 0
    for ref in results:
        ref[...] = product[at : at + ref.shape[0]]
        at += ref.shape[0]


def added(*parts):
    total = parts[0].astype(jnp.float32)
    for p in parts[1:]:
        total = total + p.astype(jnp.float32)
    return total.astype(jnp.bfloat16)


def layer(
    tokens,
    norm_gain,
    w_bgate,
    w_cgate,
    w_conv_in,
    conv_taps,
    w_query,
    w_key,
    w_value,
    sink_logits,
    conv_out_weight,
    attn_out_weight,
):
    fs = lax.axis_size("fs")
    sp = lax.axis_size("sp")
    tp = lax.axis_size("tp")
    bf16, f32 = jnp.bfloat16, jnp.float32
    rows_in = w_bgate.shape[0]
    chans = w_bgate.shape[1] // fs
    block = rows_in * fs
    b_width, out_cols = 3 * chans, 2 * chans
    in_cols = b_width + chans + 2 * HEAD
    width = in_cols + out_cols
    core, place, group = lax.axis_index("tp"), lax.axis_index("sp"), lax.axis_index("fs")
    idx = (place * tp + core).astype(jnp.int32).reshape(1)
    member = group.astype(jnp.int32).reshape(1)
    packed = pl.pallas_call(
        pack_kernel,
        out_shape=(jax.ShapeDtypeStruct((rows_in, width), bf16),) * fs,
        in_specs=[SMEM] + [VMEM] * 8,
        out_specs=(VMEM,) * fs,
        name="pack_weights",
    )(member, w_query, w_key, w_value, conv_out_weight.T, attn_out_weight.T, w_bgate, w_cgate, w_conv_in)
    mine = pl.pallas_call(
        functools.partial(turn_kernel, in_cols),
        out_shape=jax.ShapeDtypeStruct((block, width), bf16),
        in_specs=[SMEM] + [VMEM] * fs,
        out_specs=VMEM,
        scratch_shapes=[pltpu.VMEM((block, out_cols), bf16)],
        name="turn_weights",
    )(member, packed[0], *(ring(p, "fs", d) for d, p in enumerate(packed) if d > 0))
    weights = lax.all_gather(mine, ("sp", "tp"), axis=0, tiled=True)
    weights = weights.reshape(sp, tp, block, width)

    heads = chans // HEAD
    taps = lax.dynamic_slice_in_dim(conv_taps, group * chans, chans, 1).astype(f32)
    sinks = lax.dynamic_slice_in_dim(sink_logits, group * heads, heads, 0)
    small = jnp.concatenate([taps, jnp.pad(sinks[None], ((0, 0), (0, chans - heads)))], axis=0)

    widened = tokens[0].astype(f32)
    normed = (
        widened
        * lax.rsqrt(jnp.mean(widened * widened, axis=-1, keepdims=True) + EPSILON)
        * norm_gain
    ).astype(bf16)
    here, feats = normed.shape
    half = here // 2
    prev = ring(normed, "fs", 1)
    succ = ring(normed, "fs", -1)
    opp_a = ring(prev[:half], "fs", 1)
    opp_b = ring(succ[half:], "fs", -1)
    theirs = lax.ppermute(small, "tp", [(0, 1), (1, 0)])
    both = jnp.where(core == 0, jnp.stack([small, theirs]), jnp.stack([theirs, small]))
    taps, sinks = both[:, :TAPS], both[:, TAPS, :heads]
    weights, idx, taps, sinks = lax.optimization_barrier((weights, idx, taps, sinks))

    squares = out_cols // block
    pair = 2 * HEAD
    proj, kvs, edge, wout = pl.pallas_call(
        functools.partial(project_kernel, b_width),
        out_shape=(
            jax.ShapeDtypeStruct((tp, fs, here, in_cols - pair), bf16),
            jax.ShapeDtypeStruct((fs, here, tp * pair), bf16),
            jax.ShapeDtypeStruct((tp, fs, WINDOW + 32, 2 * HEAD), bf16),
            jax.ShapeDtypeStruct((tp * out_cols, feats), bf16),
        ),
        grid=(tp,),
        in_specs=[ANY] * 6,
        out_specs=(
            pl.BlockSpec((1, fs, here, in_cols - pair), lambda t: (t, 0, 0, 0)),
            pl.BlockSpec((fs, here, tp * pair), lambda t: (0, 0, 0)),
            pl.BlockSpec((tp, fs, WINDOW + 32, pair), lambda t: (0, 0, 0, 0)),
            ANY,
        ),
        scratch_shapes=[
            pltpu.VMEM((fs, here, feats), bf16),
            pltpu.VMEM((tp, sp, block, in_cols - pair), bf16),
            pltpu.VMEM((sp, block, tp * pair), bf16),
            pltpu.VMEM((tp * out_cols, feats), bf16),
            pltpu.SemaphoreType.DMA((10 + tp * squares * sp,)),
        ],
        cost_estimate=pl.CostEstimate(
            flops=2 * tp * fs * here * feats * in_cols, bytes_accessed=25_000_000, transcendentals=0
        ),
        compiler_params=pltpu.CompilerParams(dimension_semantics=("arbitrary",)),
        name="project_rows",
    )(weights, opp_a, opp_b, succ, prev, normed)
    edge = lax.ppermute(edge, ("sp", "tp"), [(i, i + 1) for i in range(sp * tp - 1)])

    def mix(tasks, pieces, arrived=()):
        seqs, blocks = zip(*tasks)
        edged = [q for q, n in tasks if n == 0]

        def part(shape, q):
            return pl.BlockSpec((tp, 1) + shape, lambda i, q=q: (0, q, 0, 0))

        return pl.pallas_call(
            functools.partial(mix_kernel, blocks, pieces, b_width),
            out_shape=tuple(jax.ShapeDtypeStruct((n, feats), bf16) for n in pieces),
            grid=(1,),
            in_specs=[SMEM, SMEM, pl.BlockSpec((tp, TAPS, chans), lambda i: (0, 0, 0)), ANY]
            + [part((here, in_cols - pair), q) for q in seqs]
            + [pl.BlockSpec((1, here, tp * pair), lambda i, q=q: (q, 0, 0)) for q in seqs]
            + [part((WINDOW + 32, 2 * HEAD), q) for q in (seqs if edged else ())]
            + [pl.BlockSpec(a.shape, lambda i: (0, 0)) for a in arrived],
            out_specs=tuple(pl.BlockSpec((n, feats), lambda i: (0, 0)) for n in pieces),
            scratch_shapes=[
                pltpu.VMEM((here, tp * out_cols), bf16),
                pltpu.VMEM((tp * out_cols, feats), bf16),
                pltpu.SemaphoreType.DMA,
            ],
            cost_estimate=pl.CostEstimate(
                flops=2 * here * feats * tp * out_cols + 600_000_000,
                bytes_accessed=8_000_000,
                transcendentals=600_000,
            ),
        )(idx, sinks, taps, wout, proj, proj, kvs, kvs, *((edge, edge) if edged else ()), *arrived)

    def sent(array, by):
        return ring(array, "fs", by)

    succ_q, prev_q, opp_q, own_q = range(4)
    low, high = mix(((succ_q, 1), (opp_q, 1)), (half, half))
    down, up_b = sent(high, -1), sent(low, 1)
    quarter = half // 2
    low_1, low_2, high = mix(((opp_q, 0), (prev_q, 0)), (quarter, quarter, half))
    up_1, up_2 = sent(low_1, 1), sent(low_2, 1)
    down_a = sent(high, -1)
    low_1, low_2, high = mix(((succ_q, 0), (prev_q, 1)), (quarter, quarter, half))
    down_b = sent(added(high, down), -1)
    up_a1, up_a2 = sent(added(low_1, up_1), 1), sent(added(low_2, up_2), 1)
    (own,) = mix(((own_q, 0), (own_q, 1)), (here,), (down_a, up_b))
    return added(own, jnp.concatenate([up_a1, up_a2, down_b], 0))[None]


def solution(mesh):
    placed = (
        P(("grp", "fs"), ("sp", "tp"), None),
        P(),
        P(("sp", "fs"), "tp"),
        P(("sp", "fs"), "tp"),
        P(("sp", "fs"), "tp"),
        P(None, "tp"),
        P(("sp", "fs"), "tp"),
        P(("sp", "fs"), "tp"),
        P(("sp", "fs"), "tp"),
        P("tp"),
        P("tp", ("sp", "fs")),
        P("tp", ("sp", "fs")),
    )
    return jax.shard_map(
        layer,
        mesh=mesh,
        in_specs=placed,
        out_specs=P(("grp", "fs"), ("sp", "tp"), None),
        check_vma=False,
    )
```

```python
import functools

import jax
import jax.numpy as jnp
from jax import lax
from jax.experimental import pallas as pl
from jax.experimental.pallas import tpu as pltpu
from jax.sharding import PartitionSpec as P


HEAD = 64
WINDOW = 128
TAPS = 3
EPSILON = 1e-06


ANY = pl.BlockSpec(memory_space=pl.ANY)
SMEM = pl.BlockSpec(memory_space=pltpu.SMEM)
VMEM = pl.BlockSpec(memory_space=pltpu.VMEM)


def ring(array, axis, by):
    size = lax.axis_size(axis)
    return lax.ppermute(array, axis, [(i, (i + by) % size) for i in range(size)])


def pack_kernel(group, wq, wk, wv, conv_t, attn_t, wb, wc, wi, *outs):
    fs = len(outs)
    chans = wq.shape[1] // fs
    for d, out in enumerate(outs):
        to = lax.rem(group[0] + d, fs)
        cut = pl.ds(pl.multiple_of(to * chans, chans), chans)
        second = to >= fs // 2
        kv = jnp.concatenate(
            [jnp.where(second, w[:, HEAD : 2 * HEAD], w[:, :HEAD]) for w in (wk, wv)], axis=1
        )
        at = 0
        for part in (wb[:, cut], wc[:, cut], wi[:, cut], wq[:, cut], kv, conv_t[:, cut], attn_t[:, cut]):
            out[:, at : at + part.shape[1]] = part
            at += part.shape[1]


def turn_kernel(in_cols, group, *refs):
    parts, out, squares = refs[:-2], refs[-2], refs[-1]
    block, width = out.shape
    rows = parts[0].shape[0]
    for d, part in enumerate(parts):
        source = lax.rem(group[0] - d + len(parts), len(parts))
        at = pl.ds(pl.multiple_of(source * rows, rows), rows)
        out[at, :in_cols] = part[:, :in_cols]
        squares[at, :] = part[:, in_cols:]
    for at in range(0, width - in_cols, block):
        out[:, in_cols + at : in_cols + at + block] = squares[:, at : at + block].T


def project_kernel(wide, weights, *refs):
    opp_a, opp_b, succ, prev, own, out, kvs, edge, wout, xs, ws, wkv, wo, sems = refs
    step = pl.program_id(0)
    half = opp_a.shape[0]
    block = weights.shape[2]
    blocks = weights.shape[0]
    main = ws.shape[3]
    pair = wkv.shape[2] // 2
    parts = (weights.shape[3] - main - pair) // block
    bf16, f32 = jnp.bfloat16, jnp.float32
    x_copies = [
        pltpu.make_async_copy(ref, xs.at[s, pl.ds(at, ref.shape[0]), :], sems.at[i])
        for i, (ref, s, at) in enumerate(
            ((succ, 0, 0), (prev, 1, 0), (opp_a, 2, 0), (opp_b, 2, half), (own, 3, 0))
        )
    ]
    w_copies = [
        pltpu.make_async_copy(weights.at[:, t, :, pl.ds(0, main)], ws.at[t], sems.at[5 + t])
        for t in range(2)
    ]
    kv_copies = [
        pltpu.make_async_copy(
            weights.at[:, t, :, pl.ds(main, pair)], wkv.at[:, :, pl.ds(t * pair, pair)], sems.at[7 + t]
        )
        for t in range(2)
    ]
    out_copies = [
        pltpu.make_async_copy(
            weights.at[j, t, :, pl.ds(main + pair + b * block, block)],
            wo.at[pl.ds((t * parts + b) * block, block), pl.ds(j * block, block)],
            sems.at[9 + (t * parts + b) * blocks + j],
        )
        for t in range(2)
        for b in range(parts)
        for j in range(blocks)
    ]
    laid_out = pltpu.make_async_copy(wo, wout, sems.at[9 + 2 * parts * blocks])

    @pl.when(step == 0)
    def _():
        for c in x_copies + w_copies[:1]:
            c.start()
        for c in x_copies + w_copies[:1]:
            c.wait()
        for c in w_copies[1:] + kv_copies + out_copies:
            c.start()

    @pl.when(step == 1)
    def _():
        for c in w_copies[1:] + kv_copies + out_copies:
            c.wait()
        laid_out.start()

    seqs, length, feats = xs.shape
    x = xs[...].reshape(seqs * length, feats)
    w = ws[step].reshape(feats, main)
    rounded = jnp.dot(x, w, preferred_element_type=f32).astype(bf16).reshape(seqs, length, main)
    out[0] = rounded
    chans = wide // 3
    for s in range(seqs):
        last = rounded[s, length - 16 :, chans:wide].astype(f32)
        gated = (last[:, :chans] * last[:, chans:]).astype(bf16)
        edge[step, s, WINDOW : WINDOW + 16, :] = gated[:, : 2 * HEAD]
        edge[step, s, WINDOW + 16 : WINDOW + 32, :] = gated[:, 2 * HEAD :]

    @pl.when(step == 1)
    def _():
        k = wkv[...].reshape(feats, 2 * pair)
        both = jnp.dot(x, k, preferred_element_type=f32).astype(bf16).reshape(seqs, length, 2 * pair)
        kvs[...] = both
        for t in range(2):
            for s in range(seqs):
                edge[t, s, 0:WINDOW, :] = both[s, length - WINDOW :, t * pair : (t + 1) * pair]
        laid_out.wait()


def mix_kernel(blocks, pieces, wide, idx, sinks, taps, wout, *refs):
    acts, wo, sem = refs[-3:]
    outs_at = len(refs) - 3 - len(pieces)
    results = refs[outs_at:-3]
    has_edge = 2 if 0 in blocks else 0
    projs, kvs, edges = refs[:2], refs[2:4], refs[4 : 4 + has_edge]
    arrived = refs[4 + has_edge : outs_at]
    wanted = pltpu.make_async_copy(wout, wo, sem)
    wanted.start()
    place = idx[0]
    chans = wide // 3
    heads = chans // HEAD
    f32, bf16 = jnp.float32, jnp.bfloat16
    q_at = wide
    pair = 2 * HEAD

    def iota(shape, dim):
        return lax.broadcasted_iota(jnp.int32, shape, dim)

    pick_kt = (iota((chans, pair), 1) == jnp.bitwise_and(iota((chans, pair), 0), HEAD - 1)).astype(bf16)
    pick_v = (iota((pair, pair), 0) == jnp.bitwise_and(iota((pair, pair), 1), HEAD - 1) + HEAD).astype(bf16)
    row = iota((WINDOW, chans), 0)
    lane = iota((WINDOW, chans), 1)
    left = iota((WINDOW, pair), 1) < HEAD
    qi, ki = iota((WINDOW, 2 * WINDOW), 0), iota((WINDOW, 2 * WINDOW), 1)
    band = (ki > qi) & (ki <= qi + WINDOW)
    first = band & ((ki >= WINDOW) | (place > 0))
    ones = jnp.ones((2 * WINDOW, pair), bf16)
    transposed = (((1,), (1,)), ((), ()))
    for slot, n in enumerate(blocks):
        at, to = n * WINDOW, slot * WINDOW
        proj, kv_rows, edge = projs[slot], kvs[slot], edges[slot] if n == 0 else None
        for side in range(2):

            def gated_rows(start, rows):
                c = proj[side, 0, start : start + rows, chans : 2 * chans].astype(f32)
                i = proj[side, 0, start : start + rows, 2 * chans : 3 * chans].astype(f32)
                return (c * i).astype(bf16).astype(f32)

            t = taps[side]
            base = side * 2 * chans
            if n == 0:
                tail = jnp.concatenate(
                    [edge[side, 0, WINDOW : WINDOW + 16, :], edge[side, 0, WINDOW + 16 : WINDOW + 32, :]],
                    axis=1,
                ).astype(f32)
            else:
                tail = gated_rows(at - 16, 16)
            before2, before1 = tail[14:15, :], tail[15:16, :]
            g = gated_rows(at, WINDOW)
            one = jnp.where(row == 0, before1, pltpu.roll(g, 1, 0))
            two = jnp.where(row == 0, before2, jnp.where(row == 1, before1, pltpu.roll(g, 2, 0)))
            convolved = two * t[0:1] + one * t[1:2] + g * t[2:3]
            out_gate = proj[side, 0, at : at + WINDOW, 0:chans].astype(f32)
            acts[to : to + WINDOW, base : base + chans] = (out_gate * convolved).astype(bf16)

            kv_cols = slice(side * pair, (side + 1) * pair)
            kv_here = kv_rows[0, at : at + WINDOW, kv_cols]
            if n == 0:
                kv_before = edge[side, 0, 0:WINDOW, :]
            else:
                kv_before = kv_rows[0, at - WINDOW : at, kv_cols]
            kv = jnp.concatenate([kv_before, kv_here], axis=0)
            keys = lax.dot_general(pick_kt, kv, transposed, preferred_element_type=f32).astype(bf16)
            values = jnp.dot(kv, pick_v, preferred_element_type=f32).astype(bf16)
            values = jnp.concatenate([values, ones], axis=1)
            q = proj[side, 0, at : at + WINDOW, q_at : q_at + chans]
            allowed = first if n == 0 else band
            outs = []
            for h in range(heads):
                qh = jnp.where((lane >= h * HEAD) & (lane < (h + 1) * HEAD), q, jnp.zeros_like(q))
                sc = jnp.dot(qh, keys, preferred_element_type=f32)
                sc = jnp.where(allowed, sc * (1.0 / 8.0), -jnp.inf)
                sink = sinks[side, h]
                m = jnp.maximum(jnp.max(sc, axis=1, keepdims=True), sink)
                e = jnp.exp(sc - m).astype(bf16)
                o = jnp.dot(e, values, preferred_element_type=f32)
                outs.append(o[:, :pair] / (o[:, pair:] + jnp.exp(sink - m)))
            for j in range(heads // 2):
                col = base + chans + j * pair
                acts[to : to + WINDOW, col : col + pair] = jnp.where(
                    left, outs[2 * j], outs[2 * j + 1]
                ).astype(bf16)

    wanted.wait()
    product = jnp.dot(acts[...], wo[...], preferred_element_type=f32)
    if arrived:
        product = product + jnp.concatenate([a[...] for a in arrived], axis=0).astype(f32)
    product = product.astype(bf16)
    at = 0
    for ref in results:
        ref[...] = product[at : at + ref.shape[0]]
        at += ref.shape[0]


def added(*parts):
    total = parts[0].astype(jnp.float32)
    for p in parts[1:]:
        total = total + p.astype(jnp.float32)
    return total.astype(jnp.bfloat16)


def layer(
    tokens,
    norm_gain,
    w_bgate,
    w_cgate,
    w_conv_in,
    conv_taps,
    w_query,
    w_key,
    w_value,
    sink_logits,
    conv_out_weight,
    attn_out_weight,
):
    fs = lax.axis_size("fs")
    sp = lax.axis_size("sp")
    tp = lax.axis_size("tp")
    bf16, f32 = jnp.bfloat16, jnp.float32
    rows_in = w_bgate.shape[0]
    chans = w_bgate.shape[1] // fs
    block = rows_in * fs
    b_width, out_cols = 3 * chans, 2 * chans
    in_cols = b_width + chans + 2 * HEAD
    width = in_cols + out_cols
    core, place, group = lax.axis_index("tp"), lax.axis_index("sp"), lax.axis_index("fs")
    idx = (place * tp + core).astype(jnp.int32).reshape(1)
    member = group.astype(jnp.int32).reshape(1)
    packed = pl.pallas_call(
        pack_kernel,
        out_shape=(jax.ShapeDtypeStruct((rows_in, width), bf16),) * fs,
        in_specs=[SMEM] + [VMEM] * 8,
        out_specs=(VMEM,) * fs,
        name="pack_weights",
    )(member, w_query, w_key, w_value, conv_out_weight.T, attn_out_weight.T, w_bgate, w_cgate, w_conv_in)
    exchanged = []
    for d in range(1, fs):
        exchanged.append(ring(packed[d], "fs", d))
    mine = pl.pallas_call(
        functools.partial(turn_kernel, in_cols),
        out_shape=jax.ShapeDtypeStruct((block, width), bf16),
        in_specs=[SMEM] + [VMEM] * fs,
        out_specs=VMEM,
        scratch_shapes=[pltpu.VMEM((block, out_cols), bf16)],
        name="turn_weights",
    )(member, packed[0], *exchanged)
    weights = lax.all_gather(mine, ("sp", "tp"), axis=0, tiled=True)
    weights = weights.reshape(sp, tp, block, width)

    heads = chans // HEAD
    taps = lax.dynamic_slice_in_dim(conv_taps, group * chans, chans, 1).astype(f32)
    sinks = lax.dynamic_slice_in_dim(sink_logits, group * heads, heads, 0)
    small = jnp.concatenate([taps, jnp.pad(sinks[None], ((0, 0), (0, chans - heads)))], axis=0)

    widened = tokens[0].astype(f32)
    normed = (
        widened
        * lax.rsqrt(jnp.mean(widened * widened, axis=-1, keepdims=True) + EPSILON)
        * norm_gain
    ).astype(bf16)
    here, feats = normed.shape
    half = here // 2
    prev = ring(normed, "fs", 1)
    succ = ring(normed, "fs", -1)
    opp_a = ring(prev[:half], "fs", 1)
    opp_b = ring(succ[half:], "fs", -1)
    theirs = lax.ppermute(small, "tp", [(0, 1), (1, 0)])
    both = jnp.where(core == 0, jnp.stack([small, theirs]), jnp.stack([theirs, small]))
    taps, sinks = both[:, :TAPS], both[:, TAPS, :heads]
    weights, idx, taps, sinks = lax.optimization_barrier((weights, idx, taps, sinks))

    squares = out_cols // block
    pair = 2 * HEAD
    proj, kvs, edge, wout = pl.pallas_call(
        functools.partial(project_kernel, b_width),
        out_shape=(
            jax.ShapeDtypeStruct((tp, fs, here, in_cols - pair), bf16),
            jax.ShapeDtypeStruct((fs, here, tp * pair), bf16),
            jax.ShapeDtypeStruct((tp, fs, WINDOW + 32, 2 * HEAD), bf16),
            jax.ShapeDtypeStruct((tp * out_cols, feats), bf16),
        ),
        grid=(tp,),
        in_specs=[ANY] * 6,
        out_specs=(
            pl.BlockSpec((1, fs, here, in_cols - pair), lambda t: (t, 0, 0, 0)),
            pl.BlockSpec((fs, here, tp * pair), lambda t: (0, 0, 0)),
            pl.BlockSpec((tp, fs, WINDOW + 32, pair), lambda t: (0, 0, 0, 0)),
            ANY,
        ),
        scratch_shapes=[
            pltpu.VMEM((fs, here, feats), bf16),
            pltpu.VMEM((tp, sp, block, in_cols - pair), bf16),
            pltpu.VMEM((sp, block, tp * pair), bf16),
            pltpu.VMEM((tp * out_cols, feats), bf16),
            pltpu.SemaphoreType.DMA((10 + tp * squares * sp,)),
        ],
        cost_estimate=pl.CostEstimate(
            flops=2 * tp * fs * here * feats * in_cols, bytes_accessed=25_000_000, transcendentals=0
        ),
        compiler_params=pltpu.CompilerParams(dimension_semantics=("arbitrary",)),
        name="project_rows",
    )(weights, opp_a, opp_b, succ, prev, normed)
    edge = lax.ppermute(edge, ("sp", "tp"), [(i, i + 1) for i in range(sp * tp - 1)])

    def mix(tasks, pieces, arrived=()):
        seqs, blocks = zip(*tasks)
        edged = [q for q, n in tasks if n == 0]

        def part(shape, q):
            return pl.BlockSpec((tp, 1) + shape, lambda i, q=q: (0, q, 0, 0))

        return pl.pallas_call(
            functools.partial(mix_kernel, blocks, pieces, b_width),
            out_shape=tuple(jax.ShapeDtypeStruct((n, feats), bf16) for n in pieces),
            grid=(1,),
            in_specs=[SMEM, SMEM, pl.BlockSpec((tp, TAPS, chans), lambda i: (0, 0, 0)), ANY]
            + [part((here, in_cols - pair), q) for q in seqs]
            + [pl.BlockSpec((1, here, tp * pair), lambda i, q=q: (q, 0, 0)) for q in seqs]
            + [part((WINDOW + 32, 2 * HEAD), q) for q in (seqs if edged else ())]
            + [pl.BlockSpec(a.shape, lambda i: (0, 0)) for a in arrived],
            out_specs=tuple(pl.BlockSpec((n, feats), lambda i: (0, 0)) for n in pieces),
            scratch_shapes=[
                pltpu.VMEM((here, tp * out_cols), bf16),
                pltpu.VMEM((tp * out_cols, feats), bf16),
                pltpu.SemaphoreType.DMA,
            ],
            cost_estimate=pl.CostEstimate(
                flops=2 * here * feats * tp * out_cols + 600_000_000,
                bytes_accessed=8_000_000,
                transcendentals=600_000,
            ),
        )(idx, sinks, taps, wout, proj, proj, kvs, kvs, *((edge, edge) if edged else ()), *arrived)

    def sent(array, by):
        return ring(array, "fs", by)

    succ_q, prev_q, opp_q, own_q = range(4)
    low, high = mix(((succ_q, 1), (opp_q, 1)), (half, half))
    down, up_b = sent(high, -1), sent(low, 1)
    quarter = half // 2
    low_1, low_2, high = mix(((opp_q, 0), (prev_q, 0)), (quarter, quarter, half))
    up_1, up_2 = sent(low_1, 1), sent(low_2, 1)
    down_a = sent(high, -1)
    low_1, low_2, high = mix(((succ_q, 0), (prev_q, 1)), (quarter, quarter, half))
    down_b = sent(added(high, down), -1)
    up_a1, up_a2 = sent(added(low_1, up_1), 1), sent(added(low_2, up_2), 1)
    (own,) = mix(((own_q, 0), (own_q, 1)), (here,), (down_a, up_b))
    return added(own, jnp.concatenate([up_a1, up_a2, down_b], 0))[None]


def solution(mesh):
    placed = (
        P(("grp", "fs"), ("sp", "tp"), None),
        P(),
        P(("sp", "fs"), "tp"),
        P(("sp", "fs"), "tp"),
        P(("sp", "fs"), "tp"),
        P(None, "tp"),
        P(("sp", "fs"), "tp"),
        P(("sp", "fs"), "tp"),
        P(("sp", "fs"), "tp"),
        P("tp"),
        P("tp", ("sp", "fs")),
        P("tp", ("sp", "fs")),
    )
    return jax.shard_map(
        layer,
        mesh=mesh,
        in_specs=placed,
        out_specs=P(("grp", "fs"), ("sp", "tp"), None),
        check_vma=False,
    )
```
